32 devices in a mesh: sp: 8 (over z, x), tp: 4 (over y, core).
Axes of the slice: x: 2, y: 2, z: 4, core: 2. Of those that a mesh axis runs over, the one named last changes fastest.
Arguments:
- query: bfloat16 [2048, 1024], P('sp', 'tp'), may hold values from -6 to 6
- forget_logits: bfloat16 [2048, 1024], P('sp', 'tp'), may hold values from -5.5 to 5.5
- written_values: bfloat16 [2048, 1024], P('sp', 'tp'), may hold values from -6 to 6
- output_gate_logits: bfloat16 [2048, 1024], P('sp', 'tp'), may hold values from -6 to 6
- forget_floor_gap: float32 [1024], P('tp'), may hold values from 0 to 0.08
- extra_log_decay: float32 [2048, 1024], P('sp', 'tp'), may hold values from -0.7 to 0
- head_norm_gain: float32 [128], replicated, may hold values from 0.1 to 1.9
- output_weight: bfloat16 [1024, 2048], P('tp'), may hold values from -0.1875 to 0.1875
- residual: bfloat16 [2048, 2048], P(('sp', 'tp')), may hold values from -6 to 6
- mixer_norm_gain: float32 [2048], replicated, may hold values from 0.1 to 1.9
- mixer_up_weight: bfloat16 [2048, 8192], P('sp', 'tp'), may hold values from -0.125 to 0.125
- mixer_down_weight: bfloat16 [8192, 2048], P(('tp', 'sp')), may hold values from -0.0625 to 0.0625
Outputs:
- layer_out: bfloat16 [2048, 2048], P(('sp', 'tp'))
The draws below stay inside these ranges and needn't reach their ends.
All inputs are finite; a program needn't handle non-finite values.
Results may differ from the reference program's by a relative error of at most 0.015.
Values may be sent and summed in bfloat16 or wider, within the bound.
A program may use at most 128 MiB of HBM per device.

```python
import jax
import jax.numpy as jnp
from jax import lax

D = 2048
FF = 8192
HEADS = 8
HEAD_K = 128
HEAD_V = 128
BLOCK = 64
TOK_DEV = 256
WIDTH = 1024
SEQ = 2048
N_SP = 8


def draw_forget_logits(key, part):
    noise_key, offset_key = jax.random.split(key)
    jitter = jnp.clip(jax.random.normal(noise_key, (SEQ, WIDTH), jnp.float32), -4.0, 4.0)
    offsets = jax.random.uniform(offset_key, (SEQ // TOK_DEV, 1, 1), jnp.float32, -1.5, 1.5)
    shifted = jitter.reshape(SEQ // TOK_DEV, TOK_DEV, WIDTH) + offsets
    return shifted.reshape(SEQ, WIDTH).astype(jnp.bfloat16)


def draw_forget_floor_gap(key, part):
    choose_key, slow_key, fast_key = jax.random.split(key, 3)
    slow_share = 0.5
    slow_head = jax.random.uniform(choose_key, (HEADS, 1), jnp.float32) < slow_share
    slow_gap = jnp.exp(jax.random.uniform(slow_key, (HEADS, HEAD_K), jnp.float32, jnp.log(0.2 / SEQ), jnp.log(1.0 / SEQ)))
    fast_gap = jnp.exp(jax.random.uniform(fast_key, (HEADS, HEAD_K), jnp.float32, jnp.log(0.02), jnp.log(0.08)))
    return jnp.where(slow_head, slow_gap, fast_gap).reshape(WIDTH).astype(jnp.float32)


def draw_extra_log_decay(key, part):
    place_key, level_key = jax.random.split(key)
    places = jax.random.randint(place_key, (3,), 0, SEQ)
    levels = jnp.log(jax.random.uniform(level_key, (3, WIDTH), jnp.float32, 0.5, 0.8))
    positions = jnp.arange(SEQ)[:, None]
    summed = jnp.zeros((SEQ, WIDTH), jnp.float32)
    for number in range(3):
        summed = summed + jnp.where(positions == places[number], levels[number][None, :], 0.0)
    return summed


def shard_levels(key, dims, pieces, low, top_value):
    level = 1.0
    for axis_at, parts in pieces:
        steps = jax.random.uniform(jax.random.fold_in(jax.random.fold_in(key, 6), axis_at), (parts,), jnp.float32, low / len(pieces), top_value / len(pieces))
        level = level * jnp.repeat(jnp.exp(steps), dims[axis_at] // parts).reshape((-1,) + (1,) * (len(dims) - 1 - axis_at))
    return level


def centred(key, dims, scale, limit, cuts=(), kind=jnp.bfloat16):
    result = scale * jax.random.normal(key, dims, jnp.float32)
    if cuts:
        result = result * shard_levels(key, dims, cuts, -0.22, 0.18)
    return jnp.clip(result, -limit, limit).astype(kind)


def setup_inputs(seed: int = 0) -> dict:
    streams_of = jax.random.split(jax.random.key(seed), 13)
    query = centred(streams_of[0], (SEQ, WIDTH), 1.0, 6.0, ((0, 8), (1, 4)))
    forget_logits = draw_forget_logits(jax.random.fold_in(streams_of[12], 71), 0)
    written_values = centred(streams_of[2], (SEQ, WIDTH), 1.0, 6.0, ((0, 8), (1, 4)))
    output_gate_logits = centred(streams_of[3], (SEQ, WIDTH), 1.0, 6.0, ((0, 8), (1, 4)))
    forget_floor_gap = draw_forget_floor_gap(jax.random.fold_in(streams_of[12], 71), 0)
    extra_log_decay = draw_extra_log_decay(jax.random.fold_in(streams_of[12], 71), 0)
    head_norm_gain = jnp.clip(1.0 + 0.18 * jax.random.normal(streams_of[6], (HEAD_V,), jnp.float32), 0.1, 1.9)
    output_weight = centred(streams_of[7], (WIDTH, D), WIDTH ** -0.5, 0.1875, ((0, 4),))
    residual = centred(streams_of[8], (SEQ, D), 1.0, 6.0, ((0, 32),))
    mixer_norm_gain = jnp.clip(1.0 + 0.18 * jax.random.normal(streams_of[9], (D,), jnp.float32), 0.1, 1.9)
    mixer_up_weight = centred(streams_of[10], (D, FF), D ** -0.5, 0.125, ((0, 8), (1, 4)))
    mixer_down_weight = centred(streams_of[11], (FF, D), FF ** -0.5, 0.0625, ((0, 32),))
    return {"query": query, "forget_logits": forget_logits, "written_values": written_values, "output_gate_logits": output_gate_logits, "forget_floor_gap": forget_floor_gap, "extra_log_decay": extra_log_decay, "head_norm_gain": head_norm_gain, "output_weight": output_weight, "residual": residual, "mixer_norm_gain": mixer_norm_gain, "mixer_up_weight": mixer_up_weight, "mixer_down_weight": mixer_down_weight}


norm_eps = 1e-06
highest_precision = lax.Precision.HIGHEST

def block_update(carry_forward_state, block_inputs):
    query_rows_block, gate_rows_block, value_rows_block, log_block = block_inputs
    cumulative_log = jnp.cumsum(log_block, axis=1)
    length = query_rows_block.shape[1]
    causal = jnp.arange(length)[:, None] >= jnp.arange(length)[None, :]
    across_blocks = jnp.einsum('dcj,djw->dcw', query_rows_block * jnp.exp(cumulative_log), carry_forward_state, precision=highest_precision)
    spread = cumulative_log[:, :, None, :] - cumulative_log[:, None, :, :]
    decay_table = jnp.exp(jnp.where(causal[None, :, :, None], spread, -jnp.inf))
    scores = jnp.einsum('htk,hsk,htsk->hts', query_rows_block, gate_rows_block, decay_table, precision=highest_precision)
    within = jnp.einsum('hts,hsv->htv', scores, value_rows_block, precision=highest_precision)
    final_log_total = cumulative_log[:, -1:, :]
    updated_state = jnp.exp(final_log_total[:, 0, :])[:, :, None] * carry_forward_state + jnp.einsum('tri,trw->tiw', gate_rows_block * jnp.exp(final_log_total - cumulative_log), value_rows_block, precision=highest_precision)
    return (updated_state, across_blocks + within)

def to_blocks(array, inner):
    length = array.shape[0]
    split_up = array.reshape(length // BLOCK, BLOCK, array.shape[1] // inner, inner)
    return jnp.transpose(split_up, (0, 2, 1, 3))

def from_blocks(blocked):
    joined = jnp.transpose(blocked, (0, 2, 1, 3))
    return joined.reshape(joined.shape[0] * joined.shape[1], joined.shape[2], joined.shape[3])

def prepare_inputs(query, forget_logits, written_values, forget_floor_gap, extra_log_decay):
    input_gate_value = forget_floor_gap[None, :] * jax.nn.sigmoid(-forget_logits.astype(jnp.float32))
    forget_log_rate = jnp.log1p(-input_gate_value) + extra_log_decay
    scaled_values = query.astype(jnp.float32) * HEAD_K ** (-0.5)
    return (scaled_values, input_gate_value, written_values.astype(jnp.float32), forget_log_rate)

def gate_out(recurrent, output_gate_logits, head_norm_gain):
    normal_part = recurrent * lax.rsqrt(lax.optimization_barrier(jnp.mean(recurrent * recurrent, axis=-1, keepdims=True)) + norm_eps)
    gating = jax.nn.silu(output_gate_logits.astype(jnp.float32)).reshape(recurrent.shape)
    mixed = normal_part * head_norm_gain * gating
    return mixed.reshape(recurrent.shape[0], -1).astype(jnp.bfloat16)

def normalize(stream, gain):
    scaled_rows = stream * lax.rsqrt(lax.optimization_barrier(jnp.mean(stream * stream, axis=-1, keepdims=True)) + norm_eps)
    return (scaled_rows * gain).astype(jnp.bfloat16)

def reference(query, forget_logits, written_values, output_gate_logits, forget_floor_gap, extra_log_decay, head_norm_gain, output_weight, residual, mixer_norm_gain, mixer_up_weight, mixer_down_weight):
    scaled_values, input_gate_value, value_rows, forget_log_rate = prepare_inputs(query, forget_logits, written_values, forget_floor_gap, extra_log_decay)
    head_count = query.shape[1] // HEAD_K
    start_state = jnp.zeros((head_count, HEAD_K, HEAD_V), jnp.float32)
    final_state, blocked = lax.scan(block_update, start_state, (to_blocks(scaled_values, HEAD_K), to_blocks(input_gate_value, HEAD_K), to_blocks(value_rows, HEAD_V), to_blocks(forget_log_rate, HEAD_K)))
    mixed = gate_out(from_blocks(blocked), output_gate_logits, head_norm_gain)
    branch = jnp.dot(mixed, output_weight, preferred_element_type=jnp.float32)
    stream = residual.astype(jnp.float32) + branch

    def channel_mix(row_block):
        normed = normalize(row_block, mixer_norm_gain)
        lifted = jnp.dot(normed, mixer_up_weight, preferred_element_type=jnp.float32)
        hidden = jnp.square(jax.nn.relu(lifted)).astype(jnp.bfloat16)
        return (row_block + jnp.dot(hidden, mixer_down_weight, preferred_element_type=jnp.float32)).astype(jnp.bfloat16)
    mapped = lax.map(channel_mix, stream.reshape(N_SP, TOK_DEV, stream.shape[1]))
    return mapped.reshape(stream.shape)
```

```python
import functools

import jax
import jax.numpy as jnp
from jax import lax
from jax.experimental import pallas as pl
from jax.experimental.pallas import tpu as pltpu
from jax.sharding import PartitionSpec as P

HEAD_K = 128
HEAD_V = 128
CHUNK = 128
OUTER = 4
LO = 2
MESH = pl.DeviceIdType.MESH
norm_eps = 1e-06


def doubling(n):
    d, out = 1, []
    while d < n:
        out.append(d)
        d *= 2
    return out


def hops(n):
    return [s * k for k in range(1, n) for s in (1, -1)]


def by_distance(n):
    return [sorted(range(n), key=lambda c: (abs(c - o), c)) for o in range(n)]


def dot_t(a, b):
    return lax.dot_general(a, b, (((1,), (1,)), ((), ())), preferred_element_type=jnp.float32)


def dot_0(a, b):
    return lax.dot_general(a, b, (((0,), (0,)), ((), ())), preferred_element_type=jnp.float32)


def dot(a, b):
    return jnp.dot(a, b, preferred_element_type=jnp.float32)


def layer_kernel(
    sp_size, tp_size, up_pieces, down_pieces,
    q_hbm, f_hbm, v_hbm, g_hbm, gap_hbm, ex_hbm, hg_hbm, wo_hbm, res_hbm, mg_hbm, up_hbm, dn_hbm,
    out_ref,
    qb, fb, vb, gb, exb, gapb, hgb, mgb, resb,
    cumb, gateb, recb, qcb, own, ownl, exc, excl, ss, sl, rs_, rl,
    mixb, mx, wob, upb, dnb,
    stream, nb, pbuf, acc, s1, r1, s2, r2, acc2, s3, r3,
    ldsem, sts, str_, lts, ltr, mxs, mxr, wos, wor, wfs, wfr, us, ur, fs, fr, dsn, dr,
    zs, zr, hs, hr, ls, lr, ls2, lr2, q1s, q1r, q2s, q2r, q3s, q3r,
):
    outer, inner, hi = OUTER, sp_size // OUTER, tp_size // LO
    sp, tp = lax.axis_index("sp"), lax.axis_index("tp")
    o, i = lax.div(sp, inner), lax.rem(sp, inner)
    h, l = lax.div(tp, LO), lax.rem(tp, LO)
    other = 1 - l
    rows, depth = res_hbm.shape
    length, local_width = q_hbm.shape
    heads = local_width // HEAD_K
    depth_part, cols = up_hbm.shape
    width = cols // outer
    down_rows = dn_hbm.shape[0]
    f32, b16 = jnp.float32, jnp.bfloat16
    steps = doubling(sp_size)

    def dev(ss_, tt):
        return (ss_, tt)

    def at_h(m):
        return lax.rem(h + m, hi)

    def from_h(m):
        return lax.rem(h - m + hi, hi)

    def at_i(m):
        return lax.rem(i + m, inner)

    def from_i(m):
        return lax.rem(i - m + inner, inner)

    def at_t(m):
        return lax.rem(tp + m, tp_size)

    def from_t(m):
        return lax.rem(tp - m + tp_size, tp_size)

    def rcopy(src, dst, ssem, rsem, device):
        return pltpu.make_async_remote_copy(
            src_ref=src, dst_ref=dst, send_sem=ssem, recv_sem=rsem,
            device_id=device, device_id_type=MESH,
        )

    loads = [
        pltpu.make_async_copy(src, dst, ldsem.at[n])
        for n, (src, dst) in enumerate(
            [
                (f_hbm, fb), (ex_hbm, exb), (gap_hbm, gapb), (v_hbm, vb), (q_hbm, qb), (g_hbm, gb),
                (hg_hbm, hgb), (mg_hbm, mgb), (res_hbm, resb),
                (wo_hbm, wob.at[tp]),
                (up_hbm.at[:, pl.ds(pl.multiple_of(o * width, width), width)], upb.at[sp]),
                (dn_hbm, dnb.at[i]),
            ]
        )
    ]
    for c in loads:
        c.start()

    barrier = pltpu.get_barrier_semaphore()
    peers = [dev(lax.rem(o + k, outer) * inner + i, tp) for k in range(1, outer)]
    peers += [dev(o * inner + at_i(m), tp) for m in range(1, inner)]
    peers += [dev(sp, at_t(m)) for m in range(1, tp_size)]
    for d in steps:
        peers += [dev(lax.rem(sp + d, sp_size), tp), dev(lax.rem(sp - d + sp_size, sp_size), tp)]
    for peer in peers:
        pl.semaphore_signal(barrier, inc=1, device_id=peer, device_id_type=MESH)
    pl.semaphore_wait(barrier, len(peers))

    up_rows = depth_part // up_pieces
    dn_rows = down_rows // down_pieces

    def up_cols(to, p):
        return up_hbm.at[
            pl.ds(p * up_rows, up_rows), pl.ds(pl.multiple_of(to * width, width), width)
        ]

    def up_place(source, p):
        return upb.at[source, pl.ds(p * up_rows, up_rows)]

    def up_send(to, p):
        return rcopy(
            up_cols(to, p), up_place(sp, p), us.at[to, p], ur.at[o, p], dev(to * inner + i, tp)
        )

    def up_recv(source, p):
        place = up_place(source * inner + i, p)
        return rcopy(place, place, us.at[source, p], ur.at[source, p], dev(source * inner + i, tp))

    def fw_send(source, p, m, src):
        return rcopy(
            src, up_place(source * inner + i, p), fs.at[source, p, m], fr.at[source, p, m],
            dev(o * inner + at_i(m), tp),
        )

    def fw_recv(source, p, m):
        place = up_place(source * inner + from_i(m), p)
        return rcopy(
            place, place, fs.at[source, p, m], fr.at[source, p, m], dev(o * inner + from_i(m), tp)
        )

    def dn_send(p, m):
        part = pl.ds(p * dn_rows, dn_rows)
        return rcopy(
            dn_hbm.at[part], dnb.at[i, part], dsn.at[p, m], dr.at[p, m],
            dev(o * inner + at_i(m), tp),
        )

    def dn_recv(p, m):
        place = dnb.at[from_i(m), pl.ds(p * dn_rows, dn_rows)]
        return rcopy(place, place, dsn.at[p, m], dr.at[p, m], dev(o * inner + from_i(m), tp))

    def inside(k):
        return (o + k >= 0) & (o + k < outer)

    def up_issue(items):
        for k, p in items:
            @pl.when(inside(k))
            def _():
                up_send(o + k, p).start()

    def own_issue(p):
        for m in range(1, inner):
            fw_send(o, p, m, up_cols(o, p)).start()

    def dn_issue(p):
        for m in range(1, inner):
            dn_send(p, m).start()

    def fw_issue(items):
        for k, p in items:
            @pl.when(inside(k))
            def _():
                up_recv(o + k, p).wait_recv()
                for m in range(1, inner):
                    fw_send(o + k, p, m, up_place((o + k) * inner + i, p)).start()

    up_list = [(k, p) for k in hops(outer) for p in range(up_pieces)]
    near = [(k, p) for k, p in up_list if abs(k) == 1]
    groups = [[(k, p) for k, p in near if p == 0], [(k, p) for k, p in near if p > 0]]
    far = [(k, p) for k, p in up_list if abs(k) > 1]
    groups += [[(k, p) for k, p in far if abs(k) == 2 and p == 0]]
    rest = [it for it in far if it not in groups[2]]

    def wo_send_l():
        return rcopy(wo_hbm, wob.at[tp], wos.at[0], wor.at[0], dev(sp, h * LO + other))

    def wo_send_h(m):
        return rcopy(wo_hbm, wob.at[tp], wos.at[m], wor.at[m], dev(sp, at_h(m) * LO + l))

    def wo_recv_h(m):
        place = wob.at[from_h(m) * LO + l]
        return rcopy(place, place, wos.at[m], wor.at[m], dev(sp, from_h(m) * LO + l))

    def wo_fw(m):
        place = wob.at[from_h(m) * LO + l]
        return rcopy(place, place, wfs.at[m], wfr.at[m], dev(sp, h * LO + other))

    wo_send_l().start()
    for m in range(1, hi):
        wo_send_h(m).start()
    own_issue(0)
    up_issue(groups[0])

    for c in loads[:4]:
        c.wait()
    gate = gapb[...] / (1.0 + jnp.exp(fb[...].astype(f32)))
    gateb[...] = gate
    log_rate = jnp.log(1.0 - gate) + exb[...]
    top = log_rate.astype(b16)
    left = log_rate - top.astype(f32)
    middle = left.astype(b16)
    low = (left - middle.astype(f32)).astype(b16)
    causal = lax.broadcasted_iota(jnp.int32, (length, length), 0) >= lax.broadcasted_iota(
        jnp.int32, (length, length), 1
    )
    ones = jnp.where(causal, 1.0, 0.0).astype(b16)
    cum = dot(ones, top) + (dot(ones, middle) + dot(ones, low))
    cumb[...] = cum
    total_log = cum[length - 1 : length, :]
    written = (gate * jnp.exp(total_log - cum)).astype(b16)
    exc[...] = jnp.zeros_like(exc)
    excl[...] = jnp.zeros_like(excl)
    sl[...] = jnp.zeros_like(sl)
    for n in range(heads):
        at = slice(n * HEAD_K, (n + 1) * HEAD_K)
        state = dot_0(vb[:, at], written[:, at])
        own[n] = state
        ss[0, n] = state.astype(b16)
        ownl[n : n + 1, :] = total_log[:, at]
        sl[0, n : n + 1, :] = total_log[:, at]

    def st_send(n):
        return rcopy(ss.at[n], rs_.at[n], sts.at[n], str_.at[n], dev(sp + steps[n], tp))

    def lt_send(n):
        return rcopy(sl.at[n], rl.at[n], lts.at[n], ltr.at[n], dev(sp + steps[n], tp))

    def step_send(n):
        @pl.when(sp + steps[n] < sp_size)
        def _():
            lt_send(n).start()
            st_send(n).start()

    def step_recv(n):
        @pl.when(sp >= steps[n])
        def _():
            lt_send(n).wait_recv()
            st_send(n).wait_recv()
            for k in range(heads):
                exc[k] = exc[k] + jnp.exp(excl[k : k + 1, :]) * rs_[n, k].astype(f32)
                excl[k : k + 1, :] = excl[k : k + 1, :] + rl[n, k : k + 1, :]

    def step_pack(n):
        for k in range(heads):
            ss[n, k] = (own[k] + jnp.exp(ownl[k : k + 1, :]) * exc[k]).astype(b16)
            sl[n, k : k + 1, :] = ownl[k : k + 1, :] + excl[k : k + 1, :]

    step_send(0)
    up_issue(groups[1])
    for p in range(1, up_pieces):
        own_issue(p)
    for p in range(down_pieces):
        dn_issue(p)

    loads[4].wait()
    scaled = qb[...].astype(f32) * HEAD_K ** (-0.5)
    qcb[...] = (scaled * jnp.exp(cum)).astype(b16)
    blocks = length // CHUNK
    tri = causal[:CHUNK, :CHUNK]
    for a in range(blocks):
        r = slice(a * CHUNK, (a + 1) * CHUNK)
        c_a, g_a, q_a = cum[r], gate[r], scaled[r]
        end = cum[(a + 1) * CHUNK - 1 : (a + 1) * CHUNK, :]
        base = cum[a * CHUNK - 1 : a * CHUNK, :] if a else jnp.zeros_like(end)
        mid = 0.5 * (end + base)
        q_d = (q_a * jnp.exp(c_a - mid)).astype(b16)
        k_d = (g_a * jnp.exp(mid - c_a)).astype(b16)
        if a:
            before = slice(0, a * CHUNK)
            q_o = (q_a * jnp.exp(c_a - base)).astype(b16)
            k_o = (gate[before] * jnp.exp(base - cum[before])).astype(b16)
        for n in range(heads):
            at = slice(n * HEAD_K, (n + 1) * HEAD_K)
            score = jnp.where(tri, dot_t(q_d[:, at], k_d[:, at]), 0.0).astype(b16)
            got = dot(score, vb[r, at])
            if a:
                score = dot_t(q_o[:, at], k_o[:, at]).astype(b16)
                got = got + dot(score, vb[before, at])
            recb[r, at] = got

    for n in range(len(steps)):
        step_recv(n)
        if n + 1 < len(steps):
            step_pack(n + 1)
            step_send(n + 1)
            if n == 0:
                up_issue(groups[2])
            if n + 2 == len(steps):
                up_issue(rest)
    if len(steps) < 2:
        up_issue(groups[2])
        up_issue(rest)

    loads[5].wait()
    loads[6].wait()
    for n in range(heads):
        at = slice(n * HEAD_K, (n + 1) * HEAD_K)
        rec = recb[:, at] + dot_t(qcb[:, at], exc[n].astype(b16))
        logits = gb[:, at].astype(f32)
        normal = rec * lax.rsqrt(jnp.mean(rec * rec, axis=-1, keepdims=True) + norm_eps)
        mixed = (normal * hgb[...] * (logits / (1.0 + jnp.exp(-logits)))).astype(b16)
        mixb[:, :, at] = mixed.reshape(tp_size, rows, HEAD_V)

    def mx_send(m):
        return rcopy(mixb.at[at_t(m)], mx.at[tp], mxs.at[m], mxr.at[m], dev(sp, at_t(m)))

    def mx_recv(m):
        place = mx.at[from_t(m)]
        return rcopy(place, place, mxs.at[m], mxr.at[m], dev(sp, from_t(m)))

    for m in range(1, tp_size):
        mx_send(m).start()
    mx[tp] = mixb[tp]
    fw_issue(near)

    for m in range(1, hi):
        wo_recv_h(m).wait_recv()
        wo_fw(m).start()
    for m in range(1, tp_size):
        mx_recv(m).wait_recv()
    for c in loads[7:10]:
        c.wait()
    wo_send_l().wait_recv()
    total = resb[...].astype(f32)
    for ll in range(LO):
        t = h * LO + ll
        total = total + dot(mx[t], wob[t])
    for m in range(1, hi):
        t = from_h(m) * LO + l
        total = total + dot(mx[t], wob[t])
    for m in range(1, hi):
        wo_fw(m).wait_recv()
        t = from_h(m) * LO + other
        total = total + dot(mx[t], wob[t])
    stream[...] = total
    scale = lax.rsqrt(jnp.mean(total * total, axis=-1, keepdims=True) + norm_eps)
    nb[o, tp] = (total * scale * mgb[...]).astype(b16)

    table = by_distance(outer)

    def chunk_at(p):
        c = 0
        for oo in range(outer):
            for pp in range(outer):
                c = jnp.where((o == oo) & (p == pp), table[oo][pp], c)
        return c

    def z_copy(c, to):
        ref = nb.at[c, tp]
        return rcopy(ref, ref, zs.at[c, to], zr.at[c], dev(to * inner + i, tp))

    def h_copy(c, m):
        ref = nb.at[c, tp]
        return rcopy(ref, ref, hs.at[c, m], hr.at[c, m], dev(sp, at_h(m) * LO + l))

    def l_copy(c):
        ref = nb.at[c, tp]
        return rcopy(ref, ref, ls.at[c], lr.at[c], dev(sp, h * LO + other))

    def l2_copy(c, m):
        ref = nb.at[c, from_h(m) * LO + l]
        return rcopy(ref, ref, ls2.at[c, m], lr2.at[c, m], dev(sp, h * LO + other))

    def pass_up(c):
        @pl.when((c <= o) & (o + 1 < outer))
        def _():
            z_copy(c, o + 1).start()

        @pl.when((c >= o) & (o > 0))
        def _():
            z_copy(c, o - 1).start()

    def spread(c):
        for m in range(1, hi):
            h_copy(c, m).start()
        l_copy(c).start()

    def gather(c):
        for m in range(1, hi):
            h_copy(c, m).wait_recv()
            l2_copy(c, m).start()

    pass_up(o)
    spread(o)
    fw_issue(groups[2] + rest)

    def ag_body(p, carry):
        c = chunk_at(p)
        z_copy(c, o).wait_recv()
        pass_up(c)
        spread(c)
        gather(chunk_at(p - 1))
        return carry

    lax.fori_loop(1, outer, ag_body, 0)
    gather(chunk_at(outer - 1))

    for c in loads[10:]:
        c.wait()
    for k in [0] + hops(outer):
        @pl.when(inside(k))
        def _():
            for p in range(up_pieces):
                for m in range(1, inner):
                    fw_recv(o + k, p, m).wait_recv()
    for p in range(down_pieces):
        for m in range(1, inner):
            dn_recv(p, m).wait_recv()

    def s1_copy(k):
        return rcopy(s1.at[k], r1.at[k], q1s.at[k], q1r.at[k], dev(sp, h * LO + other))

    def s2_copy(k, m):
        return rcopy(s2.at[k, m], r2.at[k, m], q2s.at[k, m], q2r.at[k, m], dev(sp, at_h(m) * LO + l))

    def s3_copy(c):
        return rcopy(s3.at[c], r3.at[o], q3s.at[c], q3r.at[o], dev(c * inner + i, tp))

    def s3_recv(c):
        return rcopy(r3.at[c], r3.at[c], q3s.at[c], q3r.at[c], dev(c * inner + i, tp))

    def turn(j):
        return chunk_at(outer - 1 - j)

    def body(j, carry):
        @pl.when(j < outer)
        def _():
            c = turn(j)
            l_copy(c).wait_recv()
            for m in range(1, hi):
                l2_copy(c, m).wait_recv()
            x = nb[c].reshape(tp_size * rows, depth)
            lifted = dot(x, upb[...].reshape(depth, width))
            hidden = jnp.square(jnp.maximum(lifted, 0.0)).astype(b16)
            part = dot(hidden, dnb[...].reshape(width, depth))
            pbuf[...] = part.reshape(tp_size, rows, depth)
            for hh in range(hi):
                s1[j, hh] = pbuf[hh * LO + other].astype(b16)
            s1_copy(j).start()
            for hh in range(hi):
                acc[j, hh] = pbuf[hh * LO + l]

        @pl.when((j >= 1) & (j < outer + 1))
        def _():
            k = j - 1
            s1_copy(k).wait_recv()
            for m in range(1, hi):
                to = at_h(m)
                s2[k, m] = (acc[k, to] + r1[k, to].astype(f32)).astype(b16)
                s2_copy(k, m).start()
            acc2[k] = acc[k, h] + r1[k, h].astype(f32)

        @pl.when(j >= 2)
        def _():
            k = j - 2
            v = acc2[k]
            for m in range(1, hi):
                s2_copy(k, m).wait_recv()
                v = v + r2[k, m].astype(f32)

            @pl.when(k < outer - 1)
            def _():
                c = turn(k)
                s3[c] = v.astype(b16)
                s3_copy(c).start()

            @pl.when(k == outer - 1)
            def _():
                stream[...] = stream[...] + v

        return carry

    lax.fori_loop(0, outer + 2, body, 0)
    final = stream[...]
    for k in range(1, outer):
        c = chunk_at(k)
        s3_recv(c).wait_recv()
        final = final + r3[c].astype(f32)
    out_ref[...] = final.astype(b16)

    wo_send_l().wait_send()
    for m in range(1, hi):
        wo_send_h(m).wait_send()
        wo_fw(m).wait_send()
    for m in range(1, tp_size):
        mx_send(m).wait_send()
    for n in range(len(steps)):
        @pl.when(sp + steps[n] < sp_size)
        def _():
            lt_send(n).wait_send()
            st_send(n).wait_send()
    for k, p in up_list:
        @pl.when(inside(k))
        def _():
            up_send(o + k, p).wait_send()
            for m in range(1, inner):
                fw_send(o + k, p, m, up_place((o + k) * inner + i, p)).wait_send()
    for m in range(1, inner):
        for p in range(up_pieces):
            fw_send(o, p, m, up_cols(o, p)).wait_send()
        for p in range(down_pieces):
            dn_send(p, m).wait_send()
    for c in range(outer):
        @pl.when((c <= o) & (o + 1 < outer))
        def _():
            z_copy(c, o + 1).wait_send()

        @pl.when((c >= o) & (o > 0))
        def _():
            z_copy(c, o - 1).wait_send()

        @pl.when(c != o)
        def _():
            s3_copy(c).wait_send()

        l_copy(c).wait_send()
        s1_copy(c).wait_send()
        for m in range(1, hi):
            h_copy(c, m).wait_send()
            l2_copy(c, m).wait_send()
            s2_copy(c, m).wait_send()


def on_device(
    sp_size, tp_size, query, forget_logits, written_values, output_gate_logits, forget_floor_gap,
    extra_log_decay, head_norm_gain, output_weight, residual, mixer_norm_gain, mixer_up_weight,
    mixer_down_weight,
):
    rows, depth = residual.shape
    length, local_width = query.shape
    heads = local_width // HEAD_K
    depth_part, cols = mixer_up_weight.shape
    down_rows = mixer_down_weight.shape[0]
    inner, hi = sp_size // OUTER, tp_size // LO
    width = cols // OUTER
    up_pieces = max(1, min(2, depth_part // 128))
    down_pieces = max(1, min(4, down_rows // 64))
    steps = len(doubling(sp_size))
    f32, b16 = jnp.float32, jnp.bfloat16
    dma = pltpu.SemaphoreType.DMA
    vm = pltpu.VMEM
    O = OUTER
    lrows = 8 * ((heads + 7) // 8)
    return pl.pallas_call(
        functools.partial(layer_kernel, sp_size, tp_size, up_pieces, down_pieces),
        out_shape=jax.ShapeDtypeStruct((rows, depth), b16),
        in_specs=[pl.BlockSpec(memory_space=pltpu.HBM)] * 12,
        out_specs=pl.BlockSpec(memory_space=pltpu.VMEM),
        scratch_shapes=[
            vm((length, local_width), b16), vm((length, local_width), b16),
            vm((length, local_width), b16), vm((length, local_width), b16),
            vm((length, local_width), f32),
            vm((1, local_width), f32), vm((1, HEAD_V), f32), vm((1, depth), f32),
            vm((rows, depth), b16),
            vm((length, local_width), f32), vm((length, local_width), f32),
            vm((length, local_width), f32), vm((length, local_width), b16),
            vm((heads, HEAD_V, HEAD_K), f32), vm((lrows, HEAD_K), f32),
            vm((heads, HEAD_V, HEAD_K), f32), vm((lrows, HEAD_K), f32),
            vm((steps, heads, HEAD_V, HEAD_K), b16), vm((steps, lrows, HEAD_K), f32),
            vm((steps, heads, HEAD_V, HEAD_K), b16), vm((steps, lrows, HEAD_K), f32),
            vm((tp_size, rows, local_width), b16), vm((tp_size, rows, local_width), b16),
            vm((tp_size, local_width, depth), b16),
            vm((sp_size, depth_part, width), b16),
            vm((inner, down_rows, depth), b16),
            vm((rows, depth), f32),
            vm((O, tp_size, rows, depth), b16),
            vm((tp_size, rows, depth), f32),
            vm((O, hi, rows, depth), f32),
            vm((O, hi, rows, depth), b16), vm((O, hi, rows, depth), b16),
            vm((O, hi, rows, depth), b16), vm((O, hi, rows, depth), b16),
            vm((O, rows, depth), f32),
            vm((O, rows, depth), b16), vm((O, rows, depth), b16),
            dma((12,)),
            dma((steps,)), dma((steps,)), dma((steps,)), dma((steps,)),
            dma((tp_size,)), dma((tp_size,)),
            dma((hi,)), dma((hi,)), dma((hi,)), dma((hi,)),
            dma((O, up_pieces)), dma((O, up_pieces)),
            dma((O, up_pieces, inner)), dma((O, up_pieces, inner)),
            dma((down_pieces, inner)), dma((down_pieces, inner)),
            dma((O, O)), dma((O,)),
            dma((O, hi)), dma((O, hi)),
            dma((O,)), dma((O,)), dma((O, hi)), dma((O, hi)),
            dma((O,)), dma((O,)), dma((O, hi)), dma((O, hi)),
            dma((O,)), dma((O,)),
        ],
        compiler_params=pltpu.CompilerParams(
            collective_id=0, has_side_effects=True, vmem_limit_bytes=60 * 1024 * 1024
        ),
    )(
        query, forget_logits, written_values, output_gate_logits, forget_floor_gap.reshape(1, -1),
        extra_log_decay, head_norm_gain.reshape(1, -1), output_weight, residual,
        mixer_norm_gain.reshape(1, -1), mixer_up_weight, mixer_down_weight,
    )


def solution(mesh):
    return jax.shard_map(
        functools.partial(on_device, mesh.shape["sp"], mesh.shape["tp"]),
        mesh=mesh,
        in_specs=(
            P("sp", "tp"),
            P("sp", "tp"),
            P("sp", "tp"),
            P("sp", "tp"),
            P("tp"),
            P("sp", "tp"),
            P(),
            P("tp", None),
            P(("sp", "tp"), None),
            P(),
            P("sp", "tp"),
            P(("tp", "sp"), None),
        ),
        out_specs=P(("sp", "tp"), None),
        check_vma=False,
    )
```

```python
import functools

import jax
import jax.numpy as jnp
from jax import lax
from jax.experimental import pallas as pl
from jax.experimental.pallas import tpu as pltpu
from jax.sharding import PartitionSpec as P

HEAD_K = 128
HEAD_V = 128
CHUNK = 128
OUTER = 4
LO = 2
MESH = pl.DeviceIdType.MESH
norm_eps = 1e-06


def doubling(n):
    d, out = 1, []
    while d < n:
        out.append(d)
        d *= 2
    return out


def hops(n):
    return [s * k for k in range(1, n) for s in (1, -1)]


def pieces_of(rows):
    return max(1, rows // 16)


def by_distance(n):
    return [
        sorted(range(n), key=lambda c: (abs(c - o), c if 2 * o < n else -c)) for o in range(n)
    ]


def dot_t(a, b):
    return lax.dot_general(a, b, (((1,), (1,)), ((), ())), preferred_element_type=jnp.float32)


def dot_0(a, b):
    return lax.dot_general(a, b, (((0,), (0,)), ((), ())), preferred_element_type=jnp.float32)


def dot(a, b):
    return jnp.dot(a, b, preferred_element_type=jnp.float32)


def layer_kernel(
    sp_size, tp_size, up_pieces, down_pieces,
    q_hbm, f_hbm, v_hbm, g_hbm, gap_hbm, ex_hbm, hg_hbm, wo_hbm, res_hbm, mg_hbm, up_hbm, dn_hbm,
    out_ref,
    qb, fb, vb, gb, exb, gapb, hgb, mgb, resb,
    cumb, gateb, recb, qcb, own, ownl, exc, excl, ss, sl, rs_, rl,
    mixb, mx, wob, upb, dnb, s6, r6,
    stream, nb, pbuf, acc, s1, r1, s2, r2, acc2, s3, r3,
    ldsem, sts, str_, lts, ltr, mxs, mxr, wos, wor, q6s, q6r, us, ur, fs, fr, dsn, dr,
    zs, zr, hs, hr, ls, lr, q1s, q1r, q2s, q2r, q3s, q3r,
):
    outer, inner, hi = OUTER, sp_size // OUTER, tp_size // LO
    sp, tp = lax.axis_index("sp"), lax.axis_index("tp")
    o, i = lax.div(sp, inner), lax.rem(sp, inner)
    h, l = lax.div(tp, LO), lax.rem(tp, LO)
    other = 1 - l
    rows, depth = res_hbm.shape
    length, local_width = q_hbm.shape
    heads = local_width // HEAD_K
    depth_part, cols = up_hbm.shape
    width = cols // outer
    down_rows = dn_hbm.shape[0]
    f32, b16 = jnp.float32, jnp.bfloat16
    steps = doubling(sp_size)
    fine = pieces_of(rows)
    part_rows = rows // fine

    def dev(ss_, tt):
        return (ss_, tt)

    def at_h(m):
        return lax.rem(h + m, hi)

    def from_h(m):
        return lax.rem(h - m + hi, hi)

    def at_i(m):
        return lax.rem(i + m, inner)

    def from_i(m):
        return lax.rem(i - m + inner, inner)

    def at_t(m):
        return lax.rem(tp + m, tp_size)

    def from_t(m):
        return lax.rem(tp - m + tp_size, tp_size)

    def rcopy(src, dst, ssem, rsem, device):
        return pltpu.make_async_remote_copy(
            src_ref=src, dst_ref=dst, send_sem=ssem, recv_sem=rsem,
            device_id=device, device_id_type=MESH,
        )

    loads = [
        pltpu.make_async_copy(src, dst, ldsem.at[n])
        for n, (src, dst) in enumerate(
            [
                (f_hbm, fb), (ex_hbm, exb), (gap_hbm, gapb), (v_hbm, vb), (q_hbm, qb), (g_hbm, gb),
                (hg_hbm, hgb), (mg_hbm, mgb), (res_hbm, resb),
                (wo_hbm, wob.at[l]),
                (up_hbm.at[:, pl.ds(pl.multiple_of(o * width, width), width)], upb.at[sp]),
                (dn_hbm, dnb.at[i]),
            ]
        )
    ]
    for c in loads:
        c.start()

    barrier = pltpu.get_barrier_semaphore()
    peers = [dev(lax.rem(o + k, outer) * inner + i, tp) for k in range(1, outer)]
    peers += [dev(o * inner + at_i(m), tp) for m in range(1, inner)]
    peers += [dev(sp, at_t(m)) for m in range(1, tp_size)]
    for d in steps:
        peers += [dev(lax.rem(sp + d, sp_size), tp), dev(lax.rem(sp - d + sp_size, sp_size), tp)]
    for peer in peers:
        pl.semaphore_signal(barrier, inc=1, device_id=peer, device_id_type=MESH)
    pl.semaphore_wait(barrier, len(peers))

    up_rows = depth_part // up_pieces
    dn_rows = down_rows // down_pieces

    def up_cols(to, p):
        return up_hbm.at[
            pl.ds(p * up_rows, up_rows), pl.ds(pl.multiple_of(to * width, width), width)
        ]

    def up_place(source, p):
        return upb.at[source, pl.ds(p * up_rows, up_rows)]

    def up_send(to, p):
        return rcopy(
            up_cols(to, p), up_place(sp, p), us, ur.at[o, p], dev(to * inner + i, tp)
        )

    def up_recv(source, p):
        place = up_place(source * inner + i, p)
        return rcopy(place, place, us, ur.at[source, p], dev(source * inner + i, tp))

    def fw_send(source, p, m, src):
        return rcopy(
            src, up_place(source * inner + i, p), fs, fr,
            dev(o * inner + at_i(m), tp),
        )

    def dn_send(p, m):
        part = pl.ds(p * dn_rows, dn_rows)
        return rcopy(
            dn_hbm.at[part], dnb.at[i, part], dsn, dr,
            dev(o * inner + at_i(m), tp),
        )

    def whole(ref, ssem, rsem):
        return rcopy(ref, ref, ssem, rsem, dev(sp, at_t(1)))

    fw_all = whole(upb.at[pl.ds(0, outer * (inner - 1))], fs, fr)
    dn_all = whole(dnb.at[pl.ds(0, inner - 1)], dsn, dr)
    up_all = whole(upb.at[pl.ds(0, outer - 1)], us, us)

    def inside(k):
        return (o + k >= 0) & (o + k < outer)

    def up_issue(items):
        for k, p in items:
            @pl.when(inside(k))
            def _():
                up_send(o + k, p).start()

    def own_issue(p):
        for m in range(1, inner):
            fw_send(o, p, m, up_cols(o, p)).start()

    def dn_issue(p):
        for m in range(1, inner):
            dn_send(p, m).start()

    def fw_issue(items):
        for k, p in items:
            @pl.when(inside(k))
            def _():
                up_recv(o + k, p).wait_recv()
                for m in range(1, inner):
                    fw_send(o + k, p, m, up_place((o + k) * inner + i, p)).start()

    up_list = [(k, p) for k in hops(outer)[::-1] for p in range(up_pieces)]
    near = [(k, p) for k, p in up_list if abs(k) == 1]
    far = [(k, p) for k, p in up_list if abs(k) > 1]
    falling = [(k, p) for k, p in up_list if k < 0]
    rising = [(k, p) for k, p in up_list[::-1] if k > 0]

    def piece(q):
        return pl.ds(q * part_rows, part_rows)

    def wo_copy():
        return rcopy(wo_hbm, wob.at[l], wos, wor, dev(sp, h * LO + other))

    wo_copy().start()
    up_issue(falling)
    for c in loads[:4]:
        c.wait()
    gate = gapb[...] / (1.0 + jnp.exp(fb[...].astype(f32)))
    gateb[...] = gate
    log_rate = jnp.log(1.0 - gate) + exb[...]
    top = log_rate.astype(b16)
    left = log_rate - top.astype(f32)
    middle = left.astype(b16)
    low = (left - middle.astype(f32)).astype(b16)
    causal = lax.broadcasted_iota(jnp.int32, (length, length), 0) >= lax.broadcasted_iota(
        jnp.int32, (length, length), 1
    )
    ones = jnp.where(causal, 1.0, 0.0).astype(b16)
    cum = dot(ones, top) + (dot(ones, middle) + dot(ones, low))
    cumb[...] = cum
    total_log = cum[length - 1 : length, :]
    written = (gate * jnp.exp(total_log - cum)).astype(b16)
    exc[...] = jnp.zeros_like(exc)
    excl[...] = jnp.zeros_like(excl)
    sl[...] = jnp.zeros_like(sl)
    for n in range(heads):
        at = slice(n * HEAD_K, (n + 1) * HEAD_K)
        state = dot_0(vb[:, at], written[:, at])
        own[n] = state
        ss[0, n] = state.astype(b16)
        ownl[n : n + 1, :] = total_log[:, at]
        sl[0, n : n + 1, :] = total_log[:, at]

    def st_send(n):
        return rcopy(ss.at[n], rs_.at[n], sts.at[n], str_.at[n], dev(sp + steps[n], tp))

    def lt_send(n):
        return rcopy(sl.at[n], rl.at[n], lts.at[n], ltr.at[n], dev(sp + steps[n], tp))

    def step_send(n):
        @pl.when(sp + steps[n] < sp_size)
        def _():
            lt_send(n).start()
            st_send(n).start()

    def step_recv(n):
        @pl.when(sp >= steps[n])
        def _():
            lt_send(n).wait_recv()
            st_send(n).wait_recv()
            for k in range(heads):
                exc[k] = exc[k] + jnp.exp(excl[k : k + 1, :]) * rs_[n, k].astype(f32)
                excl[k : k + 1, :] = excl[k : k + 1, :] + rl[n, k : k + 1, :]

    def step_pack(n):
        for k in range(heads):
            ss[n, k] = (own[k] + jnp.exp(ownl[k : k + 1, :]) * exc[k]).astype(b16)
            sl[n, k : k + 1, :] = ownl[k : k + 1, :] + excl[k : k + 1, :]

    step_send(0)
    for p in range(up_pieces):
        own_issue(p)
    for p in range(down_pieces):
        dn_issue(p)

    loads[4].wait()
    scaled = qb[...].astype(f32) * HEAD_K ** (-0.5)
    qcb[...] = (scaled * jnp.exp(cum)).astype(b16)
    blocks = length // CHUNK
    tri = causal[:CHUNK, :CHUNK]
    for a in range(blocks):
        r = slice(a * CHUNK, (a + 1) * CHUNK)
        c_a, g_a, q_a = cum[r], gate[r], scaled[r]
        end = cum[(a + 1) * CHUNK - 1 : (a + 1) * CHUNK, :]
        base = cum[a * CHUNK - 1 : a * CHUNK, :] if a else jnp.zeros_like(end)
        mid = 0.5 * (end + base)
        q_d = (q_a * jnp.exp(c_a - mid)).astype(b16)
        k_d = (g_a * jnp.exp(mid - c_a)).astype(b16)
        if a:
            before = slice(0, a * CHUNK)
            q_o = (q_a * jnp.exp(c_a - base)).astype(b16)
            k_o = (gate[before] * jnp.exp(base - cum[before])).astype(b16)
        for n in range(heads):
            at = slice(n * HEAD_K, (n + 1) * HEAD_K)
            score = jnp.where(tri, dot_t(q_d[:, at], k_d[:, at]), 0.0).astype(b16)
            got = dot(score, vb[r, at])
            if a:
                score = dot_t(q_o[:, at], k_o[:, at]).astype(b16)
                got = got + dot(score, vb[before, at])
            recb[r, at] = got

    for n in range(len(steps)):
        step_recv(n)
        if n + 1 < len(steps):
            step_pack(n + 1)
            step_send(n + 1)
            if n + 2 == len(steps):
                up_issue(rising)
    if len(steps) < 2:
        up_issue(rising)

    loads[5].wait()
    loads[6].wait()
    for n in range(heads):
        at = slice(n * HEAD_K, (n + 1) * HEAD_K)
        rec = recb[:, at] + dot_t(qcb[:, at], exc[n].astype(b16))
        logits = gb[:, at].astype(f32)
        normal = rec * lax.rsqrt(jnp.mean(rec * rec, axis=-1, keepdims=True) + norm_eps)
        mixed = (normal * hgb[...] * (logits / (1.0 + jnp.exp(-logits)))).astype(b16)
        mixb[:, :, at] = mixed.reshape(tp_size, rows, HEAD_V)

    def mx_copy(hh):
        return rcopy(
            mixb.at[hh * LO + other], mx.at[l, hh], mxs, mxr, dev(sp, h * LO + other)
        )

    def p6_copy(m, q):
        return rcopy(
            s6.at[m, piece(q)], r6.at[m, piece(q)], q6s, q6r.at[m - 1, q],
            dev(sp, at_h(m) * LO + l),
        )

    for hh in range(hi):
        mx_copy(hh).start()
    for hh in range(hi):
        mx[l, hh] = mixb[hh * LO + l]
    for c in loads[7:10]:
        c.wait()
    wo_copy().wait_recv()
    mx_all = whole(mx.at[0], mxs, mxr)
    mx_all.wait_recv()

    def projected(hh):
        got = dot(mx[0, hh], wob[0])
        for ll in range(1, LO):
            got = got + dot(mx[ll, hh], wob[ll])
        return got

    for m in range(1, hi):
        s6[m] = projected(at_h(m)).astype(b16)
        for q in range(fine):
            p6_copy(m, q).start()
    stream[...] = resb[...].astype(f32) + projected(h)

    table = by_distance(outer)

    def chunk_at(p):
        c = 0
        for oo in range(outer):
            for pp in range(outer):
                c = jnp.where((o == oo) & (p == pp), table[oo][pp], c)
        return c

    def z_copy(c, q, to):
        ref = nb.at[c, tp, piece(q)]
        return rcopy(ref, ref, zs.at[c, jnp.where(to > o, 1, 0)], zr.at[c, q], dev(to * inner + i, tp))

    def h_copy(c, q, m):
        ref = nb.at[c, tp, piece(q)]
        return rcopy(ref, ref, hs, hr.at[c, m - 1, q], dev(sp, at_h(m) * LO + l))

    def l_copy(c, q):
        ref = nb.at[c, tp, piece(q)]
        return rcopy(ref, ref, ls, lr.at[c], dev(sp, h * LO + other))

    def l2_copy(c, q, m):
        ref = nb.at[c, from_h(m) * LO + l, piece(q)]
        return rcopy(ref, ref, ls, lr.at[c], dev(sp, h * LO + other))

    def pass_on(c, q):
        @pl.when((c <= o) & (o + 1 < outer))
        def _():
            z_copy(c, q, o + 1).start()

        @pl.when((c >= o) & (o > 0))
        def _():
            z_copy(c, q, o - 1).start()

    def spread(c, q):
        for m in range(1, hi):
            h_copy(c, q, m).start()
        l_copy(c, q).start()

    def gather(c, q):
        for m in range(1, hi):
            h_copy(c, q, m).wait_recv()
            l2_copy(c, q, m).start()

    for q in range(fine):
        r = slice(q * part_rows, (q + 1) * part_rows)
        total = stream[r]
        for m in range(1, hi):
            p6_copy(m, q).wait_recv()
            total = total + r6[m, r].astype(f32)
        stream[r] = total
        scale = lax.rsqrt(jnp.mean(total * total, axis=-1, keepdims=True) + norm_eps)
        nb[o, tp, r] = (total * scale * mgb[...]).astype(b16)
        pass_on(o, q)
        spread(o, q)

    for p in range(1, outer):
        c = chunk_at(p)
        for q in range(fine):
            z_copy(c, q, o).wait_recv()
            pass_on(c, q)
            spread(c, q)
            gather(chunk_at(p - 1), q)
            if p == 1:
                fw_issue(([near] + [far[n :: fine - 1] for n in range(fine - 1)])[q] if fine > 1 else near + far)
    for q in range(fine):
        gather(chunk_at(outer - 1), q)

    for c in loads[10:]:
        c.wait()
    fw_all.wait_recv()
    dn_all.wait_recv()

    def s1_copy(k):
        return rcopy(s1.at[k], r1.at[k], q1s, q1r.at[k], dev(sp, h * LO + other))

    def s2_copy(k, m, q):
        return rcopy(
            s2.at[k, m, piece(q)], r2.at[k, m, piece(q)], q2s, q2r.at[k, m - 1, q],
            dev(sp, at_h(m) * LO + l),
        )

    def before(c):
        return jnp.where(c > o, o > 0, o + 1 < outer)

    def s3_copy(c, q):
        to = jnp.where(c > o, o + 1, o - 1)
        slot = jnp.where((c < o) & (c == to), outer, c)
        return rcopy(
            s3.at[c, piece(q)], r3.at[slot, piece(q)], q3s, q3r.at[slot, q],
            dev(to * inner + i, tp),
        )

    def s3_recv(slot, q):
        place = r3.at[slot, piece(q)]
        return rcopy(place, place, q3s, q3r.at[slot, q], dev(sp, at_t(1)))

    def relay(k, q):
        c = turn(k)
        r = slice(q * part_rows, (q + 1) * part_rows)

        @pl.when(before(c))
        def _():
            s3_recv(c, q).wait_recv()
            acc2[k, r] = acc2[k, r] + r3[c, r].astype(f32)

        s3[c, r] = acc2[k, r].astype(b16)
        s3_copy(c, q).start()

    def turn(j):
        return chunk_at(outer - 1 - j)

    def body(j, carry):
        @pl.when(j < outer)
        def _():
            c = turn(j)
            whole(nb.at[c, pl.ds(0, hi)], ls, lr.at[c]).wait_recv()
            x = nb[c].reshape(tp_size * rows, depth)
            lifted = dot(x, upb[...].reshape(depth, width))
            hidden = jnp.square(jnp.maximum(lifted, 0.0)).astype(b16)
            part = dot(hidden, dnb[...].reshape(width, depth))
            pbuf[...] = part.reshape(tp_size, rows, depth)
            for hh in range(hi):
                s1[j, hh] = pbuf[hh * LO + other].astype(b16)
            s1_copy(j).start()
            for hh in range(hi):
                acc[j, hh] = pbuf[hh * LO + l]

        @pl.when(j >= 1)
        def _():
            k = j - 1
            s1_copy(k).wait_recv()
            for m in range(1, hi):
                to = at_h(m)
                for q in range(fine):
                    r = slice(q * part_rows, (q + 1) * part_rows)
                    s2[k, m, r] = (acc[k, to, r] + r1[k, to, r].astype(f32)).astype(b16)
                    s2_copy(k, m, q).start()
            acc2[k] = acc[k, h] + r1[k, h].astype(f32)

        return carry

    lax.fori_loop(0, outer + 1, body, 0)

    for k in range(outer):
        for q in range(fine):
            r = slice(q * part_rows, (q + 1) * part_rows)
            v = acc2[k, r]
            for m in range(1, hi):
                s2_copy(k, m, q).wait_recv()
                v = v + r2[k, m, r].astype(f32)
            acc2[k, r] = v
            if 0 < k < outer - 1:
                @pl.when(before(turn(k - 1)))
                def _():
                    relay(k - 1, q)
            if k == outer - 2:
                relay(k, q)
            elif k < outer - 2:
                @pl.when(jnp.logical_not(before(turn(k))))
                def _():
                    relay(k, q)

    for q in range(fine):
        r = slice(q * part_rows, (q + 1) * part_rows)
        final = stream[r] + acc2[outer - 1, r]
        stream[r] = final

        @pl.when(o > 0)
        def _():
            s3_recv(o, q).wait_recv()
            stream[r] = stream[r] + r3[o, r].astype(f32)

        @pl.when(o + 1 < outer)
        def _():
            s3_recv(outer, q).wait_recv()
            stream[r] = stream[r] + r3[outer, r].astype(f32)

        out_ref[r] = stream[r].astype(b16)

    wo_copy().wait_send()
    mx_all.wait_send()
    whole(s6.at[pl.ds(0, hi - 1)], q6s, q6s).wait_send()
    for n in range(len(steps)):
        @pl.when(sp + steps[n] < sp_size)
        def _():
            lt_send(n).wait_send()
            st_send(n).wait_send()
    up_all.wait_send()
    fw_all.wait_send()
    dn_all.wait_send()
    for c in range(outer):
        @pl.when((c <= o) & (o + 1 < outer))
        def _():
            whole(nb.at[c, tp], zs.at[c, 1], zs.at[c, 1]).wait_send()

        @pl.when((c >= o) & (o > 0))
        def _():
            whole(nb.at[c, tp], zs.at[c, 0], zs.at[c, 0]).wait_send()

    whole(s1.at[:, pl.ds(0, hi - 1)], hs, hs).wait_send()
    whole(s1, ls, ls).wait_send()
    whole(s1, q1s, q1s).wait_send()
    whole(s2.at[:, pl.ds(0, hi - 1)], q2s, q2s).wait_send()
    whole(s3.at[pl.ds(0, outer - 1)], q3s, q3s).wait_send()


def on_device(
    sp_size, tp_size, query, forget_logits, written_values, output_gate_logits, forget_floor_gap,
    extra_log_decay, head_norm_gain, output_weight, residual, mixer_norm_gain, mixer_up_weight,
    mixer_down_weight,
):
    rows, depth = residual.shape
    length, local_width = query.shape
    heads = local_width // HEAD_K
    depth_part, cols = mixer_up_weight.shape
    down_rows = mixer_down_weight.shape[0]
    inner, hi = sp_size // OUTER, tp_size // LO
    width = cols // OUTER
    up_pieces = max(1, min(2, depth_part // 128))
    down_pieces = max(1, min(4, down_rows // 64))
    steps = len(doubling(sp_size))
    f32, b16 = jnp.float32, jnp.bfloat16
    dma = pltpu.SemaphoreType.DMA
    vm = pltpu.VMEM
    O, F = OUTER, pieces_of(rows)
    lrows = 8 * ((heads + 7) // 8)
    return pl.pallas_call(
        functools.partial(layer_kernel, sp_size, tp_size, up_pieces, down_pieces),
        out_shape=jax.ShapeDtypeStruct((rows, depth), b16),
        in_specs=[pl.BlockSpec(memory_space=pltpu.HBM)] * 12,
        out_specs=pl.BlockSpec(memory_space=pltpu.VMEM),
        scratch_shapes=[
            vm((length, local_width), b16), vm((length, local_width), b16),
            vm((length, local_width), b16), vm((length, local_width), b16),
            vm((length, local_width), f32),
            vm((1, local_width), f32), vm((1, HEAD_V), f32), vm((1, depth), f32),
            vm((rows, depth), b16),
            vm((length, local_width), f32), vm((length, local_width), f32),
            vm((length, local_width), f32), vm((length, local_width), b16),
            vm((heads, HEAD_V, HEAD_K), f32), vm((lrows, HEAD_K), f32),
            vm((heads, HEAD_V, HEAD_K), f32), vm((lrows, HEAD_K), f32),
            vm((steps, heads, HEAD_V, HEAD_K), b16), vm((steps, lrows, HEAD_K), f32),
            vm((steps, heads, HEAD_V, HEAD_K), b16), vm((steps, lrows, HEAD_K), f32),
            vm((tp_size, rows, local_width), b16), vm((LO, hi, rows, local_width), b16),
            vm((LO, local_width, depth), b16),
            vm((sp_size, depth_part, width), b16),
            vm((inner, down_rows, depth), b16),
            vm((hi, rows, depth), b16), vm((hi, rows, depth), b16),
            vm((rows, depth), f32),
            vm((O, tp_size, rows, depth), b16),
            vm((tp_size, rows, depth), f32),
            vm((O, hi, rows, depth), f32),
            vm((O, hi, rows, depth), b16), vm((O, hi, rows, depth), b16),
            vm((O, hi, rows, depth), b16), vm((O, hi, rows, depth), b16),
            vm((O, rows, depth), f32),
            vm((O, rows, depth), b16), vm((O + 1, rows, depth), b16),
            dma((12,)),
            dma((steps,)), dma((steps,)), dma((steps,)), dma((steps,)),
            dma, dma, dma, dma,
            dma, dma((hi - 1, F)),
            dma, dma((O, up_pieces)),
            dma, dma, dma, dma,
            dma((O, 2)), dma((O, F)),
            dma, dma((O, hi - 1, F)),
            dma, dma((O,)),
            dma, dma((O,)), dma, dma((O, hi - 1, F)),
            dma, dma((O + 1, F)),
        ],
        compiler_params=pltpu.CompilerParams(
            collective_id=0, has_side_effects=True, vmem_limit_bytes=60 * 1024 * 1024
        ),
    )(
        query, forget_logits, written_values, output_gate_logits, forget_floor_gap.reshape(1, -1),
        extra_log_decay, head_norm_gain.reshape(1, -1), output_weight, residual,
        mixer_norm_gain.reshape(1, -1), mixer_up_weight, mixer_down_weight,
    )


def solution(mesh):
    return jax.shard_map(
        functools.partial(on_device, mesh.shape["sp"], mesh.shape["tp"]),
        mesh=mesh,
        in_specs=(
            P("sp", "tp"),
            P("sp", "tp"),
            P("sp", "tp"),
            P("sp", "tp"),
            P("tp"),
            P("sp", "tp"),
            P(),
            P("tp", None),
            P(("sp", "tp"), None),
            P(),
            P("sp", "tp"),
            P(("tp", "sp"), None),
        ),
        out_specs=P(("sp", "tp"), None),
        check_vma=False,
    )
```

```python
import functools

import jax
import jax.numpy as jnp
from jax import lax
from jax.experimental import pallas as pl
from jax.experimental.pallas import tpu as pltpu
from jax.sharding import PartitionSpec as P

HEAD_K = 128
HEAD_V = 128
CHUNK = 128
OUTER = 4
LO = 2
MESH = pl.DeviceIdType.MESH
norm_eps = 1e-06


def doubling(n):
    d, out = 1, []
    while d < n:
        out.append(d)
        d *= 2
    return out


def hops(n):
    return [s * k for k in range(1, n) for s in (1, -1)]


def pieces_of(rows):
    return max(1, rows // 16)


def halves_of(rows):
    return max(1, rows // 32)


def by_distance(n):
    return [
        sorted(range(n), key=lambda c: (abs(c - o), c if 2 * o < n else -c)) for o in range(n)
    ]


def dot_t(a, b):
    return lax.dot_general(a, b, (((1,), (1,)), ((), ())), preferred_element_type=jnp.float32)


def dot_0(a, b):
    return lax.dot_general(a, b, (((0,), (0,)), ((), ())), preferred_element_type=jnp.float32)


def dot(a, b):
    return jnp.dot(a, b, preferred_element_type=jnp.float32)


def layer_kernel(
    sp_size, tp_size, up_pieces, down_pieces,
    q_hbm, f_hbm, v_hbm, g_hbm, gap_hbm, ex_hbm, hg_hbm, wo_hbm, res_hbm, mg_hbm, up_hbm, dn_hbm,
    out_ref,
    qb, fb, vb, gb, exb, gapb, hgb, mgb, resb,
    cumb, gateb, recb, qcb, own, ownl, exc, excl, ss, sl, rs_, rl,
    mixb, mx, wob, upb, dnb, s6, r6,
    stream, nb, hid, pbuf, acc, s1, r1, s2, r2, acc2, s3, r3,
    ldsem, sts, str_, lts, ltr, mxs, mxr, wos, wor, q6s, q6r, us, ur, fs, fr, dsn, dr,
    zs, zr, hs, hr, ls, lr, q1s, q1r, q2s, q2r, q3s, q3r,
):
    outer, inner, hi = OUTER, sp_size // OUTER, tp_size // LO
    sp, tp = lax.axis_index("sp"), lax.axis_index("tp")
    o, i = lax.div(sp, inner), lax.rem(sp, inner)
    h, l = lax.div(tp, LO), lax.rem(tp, LO)
    other = 1 - l
    rows, depth = res_hbm.shape
    length, local_width = q_hbm.shape
    heads = local_width // HEAD_K
    depth_part, cols = up_hbm.shape
    width = cols // outer
    down_rows = dn_hbm.shape[0]
    f32, b16 = jnp.float32, jnp.bfloat16
    steps = doubling(sp_size)
    fine = pieces_of(rows)
    part_rows = rows // fine
    coarse = halves_of(rows)
    sum_rows = rows // coarse
    half = depth // 2

    def dev(ss_, tt):
        return (ss_, tt)

    def at_h(m):
        return lax.rem(h + m, hi)

    def from_h(m):
        return lax.rem(h - m + hi, hi)

    def at_i(m):
        return lax.rem(i + m, inner)

    def from_i(m):
        return lax.rem(i - m + inner, inner)

    def at_t(m):
        return lax.rem(tp + m, tp_size)

    def from_t(m):
        return lax.rem(tp - m + tp_size, tp_size)

    def rcopy(src, dst, ssem, rsem, device):
        return pltpu.make_async_remote_copy(
            src_ref=src, dst_ref=dst, send_sem=ssem, recv_sem=rsem,
            device_id=device, device_id_type=MESH,
        )

    loads = [
        pltpu.make_async_copy(src, dst, ldsem.at[n])
        for n, (src, dst) in enumerate(
            [
                (f_hbm, fb), (ex_hbm, exb), (gap_hbm, gapb), (v_hbm, vb), (q_hbm, qb), (g_hbm, gb),
                (hg_hbm, hgb), (mg_hbm, mgb), (res_hbm, resb),
                (wo_hbm, wob.at[l]),
                (up_hbm.at[:, pl.ds(pl.multiple_of(o * width, width), width)], upb.at[sp]),
                (dn_hbm, dnb.at[i]),
            ]
        )
    ]
    for c in loads:
        c.start()

    barrier = pltpu.get_barrier_semaphore()
    peers = [dev(lax.rem(o + k, outer) * inner + i, tp) for k in range(1, outer)]
    peers += [dev(o * inner + at_i(m), tp) for m in range(1, inner)]
    peers += [dev(sp, at_t(m)) for m in range(1, tp_size)]
    for d in steps:
        peers += [dev(lax.rem(sp + d, sp_size), tp), dev(lax.rem(sp - d + sp_size, sp_size), tp)]
    for peer in peers:
        pl.semaphore_signal(barrier, inc=1, device_id=peer, device_id_type=MESH)
    pl.semaphore_wait(barrier, len(peers))

    up_rows = depth_part // up_pieces
    dn_rows = down_rows // down_pieces

    def up_cols(to, p):
        return up_hbm.at[
            pl.ds(p * up_rows, up_rows), pl.ds(pl.multiple_of(to * width, width), width)
        ]

    def up_place(source, p):
        return upb.at[source, pl.ds(p * up_rows, up_rows)]

    def up_send(to, p):
        return rcopy(
            up_cols(to, p), up_place(sp, p), us, ur.at[o, p], dev(to * inner + i, tp)
        )

    def up_recv(source, p):
        place = up_place(source * inner + i, p)
        return rcopy(place, place, us, ur.at[source, p], dev(source * inner + i, tp))

    def fw_send(source, p, m, src):
        return rcopy(
            src, up_place(source * inner + i, p), fs, fr,
            dev(o * inner + at_i(m), tp),
        )

    def dn_send(n, p, m):
        part, at = pl.ds(p * dn_rows, dn_rows), pl.ds(n * half, half)
        return rcopy(
            dn_hbm.at[part, at], dnb.at[i, part, at], dsn, dr.at[n], dev(o * inner + at_i(m), tp)
        )

    def whole(ref, ssem, rsem):
        return rcopy(ref, ref, ssem, rsem, dev(sp, at_t(1)))

    fw_all = whole(upb.at[pl.ds(0, outer * (inner - 1))], fs, fr)
    dn_all = whole(dnb.at[pl.ds(0, inner - 1)], dsn, dsn)

    def dn_half(n):
        return whole(dnb.at[pl.ds(0, inner - 1), :, pl.ds(n * half, half)], dsn, dr.at[n])

    up_all = whole(upb.at[pl.ds(0, outer - 1)], us, us)

    def inside(k):
        return (o + k >= 0) & (o + k < outer)

    def up_issue(items):
        for k, p in items:
            @pl.when(inside(k))
            def _():
                up_send(o + k, p).start()

    def own_issue(p):
        for m in range(1, inner):
            fw_send(o, p, m, up_cols(o, p)).start()

    def dn_issue(items):
        for n, p in items:
            for m in range(1, inner):
                dn_send(n, p, m).start()

    dn_list = [(n, p) for n in range(2) for p in range(down_pieces)]

    def fw_issue(items):
        for k, p in items:
            @pl.when(inside(k))
            def _():
                up_recv(o + k, p).wait_recv()
                for m in range(1, inner):
                    fw_send(o + k, p, m, up_place((o + k) * inner + i, p)).start()

    up_list = [(k, p) for k in hops(outer)[::-1] for p in range(up_pieces)]
    near = [(k, p) for k, p in up_list if abs(k) == 1]
    far = [(k, p) for k, p in up_list if abs(k) > 1]
    falling = [(k, p) for k, p in up_list if k < 0]
    rising = [(k, p) for k, p in near if k > 0]
    rising_far = [(k, p) for k, p in far if k > 0]

    def piece(q):
        return pl.ds(q * part_rows, part_rows)

    def wo_copy():
        return rcopy(wo_hbm, wob.at[l], wos, wor, dev(sp, h * LO + other))

    wo_copy().start()
    up_issue(falling)
    for c in loads[:4]:
        c.wait()
    gate = gapb[...] / (1.0 + jnp.exp(fb[...].astype(f32)))
    gateb[...] = gate
    log_rate = jnp.log(1.0 - gate) + exb[...]
    top = log_rate.astype(b16)
    left = log_rate - top.astype(f32)
    middle = left.astype(b16)
    low = (left - middle.astype(f32)).astype(b16)
    causal = lax.broadcasted_iota(jnp.int32, (length, length), 0) >= lax.broadcasted_iota(
        jnp.int32, (length, length), 1
    )
    ones = jnp.where(causal, 1.0, 0.0).astype(b16)
    cum = dot(ones, top) + (dot(ones, middle) + dot(ones, low))
    cumb[...] = cum
    total_log = cum[length - 1 : length, :]
    written = (gate * jnp.exp(total_log - cum)).astype(b16)
    exc[...] = jnp.zeros_like(exc)
    excl[...] = jnp.zeros_like(excl)
    sl[...] = jnp.zeros_like(sl)
    for n in range(heads):
        at = slice(n * HEAD_K, (n + 1) * HEAD_K)
        state = dot_0(vb[:, at], written[:, at])
        own[n] = state
        ss[0, n] = state.astype(b16)
        ownl[n : n + 1, :] = total_log[:, at]
        sl[0, n : n + 1, :] = total_log[:, at]

    def st_send(n):
        return rcopy(ss.at[n], rs_.at[n], sts.at[n], str_.at[n], dev(sp + steps[n], tp))

    def lt_send(n):
        return rcopy(sl.at[n], rl.at[n], lts.at[n], ltr.at[n], dev(sp + steps[n], tp))

    def step_send(n):
        @pl.when(sp + steps[n] < sp_size)
        def _():
            lt_send(n).start()
            st_send(n).start()

    def step_recv(n):
        @pl.when(sp >= steps[n])
        def _():
            lt_send(n).wait_recv()
            st_send(n).wait_recv()
            for k in range(heads):
                exc[k] = exc[k] + jnp.exp(excl[k : k + 1, :]) * rs_[n, k].astype(f32)
                excl[k : k + 1, :] = excl[k : k + 1, :] + rl[n, k : k + 1, :]

    def step_pack(n):
        for k in range(heads):
            ss[n, k] = (own[k] + jnp.exp(ownl[k : k + 1, :]) * exc[k]).astype(b16)
            sl[n, k : k + 1, :] = ownl[k : k + 1, :] + excl[k : k + 1, :]

    step_send(0)
    up_issue(rising[:1])
    for p in range(up_pieces):
        own_issue(p)
    dn_issue(dn_list[:-1])

    loads[4].wait()
    scaled = qb[...].astype(f32) * HEAD_K ** (-0.5)
    qcb[...] = (scaled * jnp.exp(cum)).astype(b16)
    blocks = length // CHUNK
    tri = causal[:CHUNK, :CHUNK]
    for a in range(blocks):
        r = slice(a * CHUNK, (a + 1) * CHUNK)
        c_a, g_a, q_a = cum[r], gate[r], scaled[r]
        end = cum[(a + 1) * CHUNK - 1 : (a + 1) * CHUNK, :]
        base = cum[a * CHUNK - 1 : a * CHUNK, :] if a else jnp.zeros_like(end)
        mid = 0.5 * (end + base)
        q_d = (q_a * jnp.exp(c_a - mid)).astype(b16)
        k_d = (g_a * jnp.exp(mid - c_a)).astype(b16)
        if a:
            before = slice(0, a * CHUNK)
            q_o = (q_a * jnp.exp(c_a - base)).astype(b16)
            k_o = (gate[before] * jnp.exp(base - cum[before])).astype(b16)
        for n in range(heads):
            at = slice(n * HEAD_K, (n + 1) * HEAD_K)
            score = jnp.where(tri, dot_t(q_d[:, at], k_d[:, at]), 0.0).astype(b16)
            got = dot(score, vb[r, at])
            if a:
                score = dot_t(q_o[:, at], k_o[:, at]).astype(b16)
                got = got + dot(score, vb[before, at])
            recb[r, at] = got

    for n in range(len(steps)):
        step_recv(n)
        if n + 1 < len(steps):
            step_pack(n + 1)
            step_send(n + 1)
            if n == 0:
                up_issue(rising[1:])
            if n + 2 == len(steps):
                @pl.when(o > 0)
                def _():
                    up_issue(rising_far)
    if len(steps) < 2:
        up_issue(rising[1:])

        @pl.when(o > 0)
        def _():
            up_issue(rising_far)

    loads[5].wait()
    loads[6].wait()
    for n in range(heads):
        at = slice(n * HEAD_K, (n + 1) * HEAD_K)
        rec = recb[:, at] + dot_t(qcb[:, at], exc[n].astype(b16))
        logits = gb[:, at].astype(f32)
        normal = rec * lax.rsqrt(jnp.mean(rec * rec, axis=-1, keepdims=True) + norm_eps)
        mixed = (normal * hgb[...] * (logits / (1.0 + jnp.exp(-logits)))).astype(b16)
        mixb[:, :, at] = mixed.reshape(tp_size, rows, HEAD_V)

    def mx_copy(hh):
        return rcopy(
            mixb.at[hh * LO + other], mx.at[l, hh], mxs, mxr, dev(sp, h * LO + other)
        )

    def p6_copy(m, q):
        return rcopy(
            s6.at[m, piece(q)], r6.at[m, piece(q)], q6s, q6r.at[m - 1, q],
            dev(sp, at_h(m) * LO + l),
        )

    for hh in range(hi):
        mx_copy(hh).start()
    for hh in range(hi):
        mx[l, hh] = mixb[hh * LO + l]
    for c in loads[7:10]:
        c.wait()
    wo_copy().wait_recv()
    mx_all = whole(mx.at[0], mxs, mxr)
    mx_all.wait_recv()

    def projected(hh):
        got = dot(mx[0, hh], wob[0])
        for ll in range(1, LO):
            got = got + dot(mx[ll, hh], wob[ll])
        return got

    for m in range(1, hi):
        s6[m] = projected(at_h(m)).astype(b16)
        for q in range(fine):
            p6_copy(m, q).start()
    stream[...] = resb[...].astype(f32) + projected(h)

    table = by_distance(outer)

    def chunk_at(p):
        c = 0
        for oo in range(outer):
            for pp in range(outer):
                c = jnp.where((o == oo) & (p == pp), table[oo][pp], c)
        return c

    def z_copy(c, q, to):
        ref = nb.at[c, tp, piece(q)]
        return rcopy(ref, ref, zs.at[c, jnp.where(to > o, 1, 0)], zr.at[c, q], dev(to * inner + i, tp))

    def h_copy(c, q, m):
        ref = nb.at[c, tp, piece(q)]
        return rcopy(ref, ref, hs, hr.at[c, m - 1, q], dev(sp, at_h(m) * LO + l))

    def l_copy(c, q):
        ref = nb.at[c, tp, piece(q)]
        return rcopy(ref, ref, ls, lr.at[c], dev(sp, h * LO + other))

    def l2_copy(c, q, m):
        ref = nb.at[c, from_h(m) * LO + l, piece(q)]
        return rcopy(ref, ref, ls, lr.at[c], dev(sp, h * LO + other))

    def pass_on(c, q):
        @pl.when((c <= o) & (o + 1 < outer))
        def _():
            z_copy(c, q, o + 1).start()

        @pl.when((c >= o) & (o > 0))
        def _():
            z_copy(c, q, o - 1).start()

    def spread(c, q):
        for m in range(1, hi):
            h_copy(c, q, m).start()
        l_copy(c, q).start()

    def gather(c, q):
        for m in range(1, hi):
            h_copy(c, q, m).wait_recv()
            l2_copy(c, q, m).start()

    for q in range(fine):
        r = slice(q * part_rows, (q + 1) * part_rows)
        total = stream[r]
        for m in range(1, hi):
            p6_copy(m, q).wait_recv()
            total = total + r6[m, r].astype(f32)
        stream[r] = total
        scale = lax.rsqrt(jnp.mean(total * total, axis=-1, keepdims=True) + norm_eps)
        nb[o, tp, r] = (total * scale * mgb[...]).astype(b16)
        pass_on(o, q)
        spread(o, q)

    @pl.when(o == 0)
    def _():
        up_issue(rising_far)

    for p in range(1, outer):
        c = chunk_at(p)
        for q in range(fine):
            z_copy(c, q, o).wait_recv()
            pass_on(c, q)
            spread(c, q)
            gather(chunk_at(p - 1), q)
            if p == 1 and q == 0:
                fw_issue(near)
            if p == 1 and q == fine // 2:
                fw_issue([it for it in far if it[0] > 0])
        if p == 1:
            fw_issue([it for it in far if it[0] < 0])
            dn_issue(dn_list[-1:])
    def gather_last():
        for q in range(fine):
            gather(chunk_at(outer - 1), q)

    for c in loads[10:]:
        c.wait()
    fw_all.wait_recv()
    dn_half(0).wait_recv()

    def s1_copy(k):
        return rcopy(s1.at[k], r1.at[k], q1s, q1r.at[k], dev(sp, h * LO + other))

    def rows_of(q):
        return slice(q * sum_rows, (q + 1) * sum_rows)

    def s2_copy(k, m, q):
        r = pl.ds(q * sum_rows, sum_rows)
        return rcopy(
            s2.at[k, m - 1, r], r2.at[k, m - 1, r], q2s, q2r.at[k, m - 1, q],
            dev(sp, at_h(m) * LO + l),
        )

    def before(c):
        return jnp.where(c > o, o > 0, o + 1 < outer)

    def s3_copy(n, c, q):
        to = jnp.where(c > o, o + 1, o - 1)
        slot = jnp.where((c < o) & (c == to), outer, c)
        r = pl.ds(q * sum_rows, sum_rows)
        return rcopy(
            s3.at[n, c, r], r3.at[n, slot, r], q3s, q3r.at[n, slot, q], dev(to * inner + i, tp)
        )

    def s3_recv(n, slot, q):
        place = r3.at[n, slot, pl.ds(q * sum_rows, sum_rows)]
        return rcopy(place, place, q3s, q3r.at[n, slot, q], dev(sp, at_t(1)))

    def relay(k, q):
        n, c, r = half_of(k), turn(k), rows_of(q)

        @pl.when(before(c))
        def _():
            s3_recv(n, c, q).wait_recv()
            acc2[k, r] = acc2[k, r] + r3[n, c, r].astype(f32)

        s3[n, c, r] = acc2[k, r].astype(b16)
        s3_copy(n, c, q).start()

    slots, lag = 2 * outer, 3

    def turn(j):
        p = jnp.where((j == 0) | (j == slots - 3), 1, outer - 1 - (j - 1) // 2)
        return chunk_at(jnp.where(j >= slots - 2, 0, p))

    def half_of(j):
        return jnp.where(j >= slots - 3, jnp.where(j == slots - 2, 0, 1), jnp.where(j == 0, 0, lax.rem(j + 1, 2)))

    def send_sums(k):
        s1_copy(k).wait_recv()
        for m in range(1, hi):
            to = at_h(m)
            for q in range(coarse):
                r = rows_of(q)
                s2[k, m - 1, r] = (acc[k, to, r] + r1[k, to, r].astype(f32)).astype(b16)
                s2_copy(k, m, q).start()
        acc2[k] = acc[k, h] + r1[k, h].astype(f32)

    def collect(k):
        for q in range(coarse):
            r = rows_of(q)
            v = acc2[k, r]
            for m in range(1, hi):
                s2_copy(k, m, q).wait_recv()
                v = v + r2[k, m - 1, r].astype(f32)
            acc2[k, r] = v

            @pl.when((k < slots - 2) & jnp.logical_not(before(turn(k))))
            def _():
                relay(k, q)

            @pl.when((k == slots - 3) & before(turn(0)))
            def _():
                relay(0, q)

            @pl.when((k >= 2) & (k < slots - 1) & before(turn(k - 1)))
            def _():
                relay(k - 1, q)

    def body(j, carry):
        @pl.when(j == 1)
        def _():
            send_sums(0)
            gather_last()

        @pl.when(j < slots)
        def _():
            c = turn(j)

            @pl.when((j == 0) | (j == slots - 2) | ((j < slots - 3) & (lax.rem(j, 2) == 1)))
            def _():
                whole(nb.at[c, pl.ds(0, hi)], ls, lr.at[c]).wait_recv()
                x = nb[c].reshape(tp_size * rows, depth)
                lifted = dot(x, upb[...].reshape(depth, width))
                hid[c] = jnp.square(jnp.maximum(lifted, 0.0)).astype(b16)

            @pl.when(j == 2)
            def _():
                dn_half(1).wait_recv()

            at = pl.ds(pl.multiple_of(half_of(j) * half, half), half)
            part = dot(hid[c], dnb[:, :, at].reshape(width, half))
            pbuf[...] = part.reshape(tp_size, rows, half)
            for hh in range(hi):
                s1[j, hh] = pbuf[hh * LO + other].astype(b16)
            s1_copy(j).start()
            for hh in range(hi):
                acc[j, hh] = pbuf[hh * LO + l]

        @pl.when((j >= 2) & (j < slots + 1))
        def _():
            send_sums(j - 1)

        @pl.when(j >= lag)
        def _():
            collect(j - lag)

        return carry

    lax.fori_loop(0, slots + lag, body, 0)

    for n in range(2):
        at = slice(n * half, (n + 1) * half)
        mine = slots - 2 + n
        for q in range(coarse):
            r = rows_of(q)

            @pl.when(o > 0)
            def _():
                s3_recv(n, o, q).wait_recv()
                acc2[mine, r] = acc2[mine, r] + r3[n, o, r].astype(f32)

            @pl.when(o + 1 < outer)
            def _():
                s3_recv(n, outer, q).wait_recv()
                acc2[mine, r] = acc2[mine, r] + r3[n, outer, r].astype(f32)

            out_ref[r, at] = (stream[r, at] + acc2[mine, r]).astype(b16)

    wo_copy().wait_send()
    mx_all.wait_send()
    whole(s6.at[pl.ds(0, hi - 1)], q6s, q6s).wait_send()
    for n in range(len(steps)):
        @pl.when(sp + steps[n] < sp_size)
        def _():
            lt_send(n).wait_send()
            st_send(n).wait_send()
    up_all.wait_send()
    fw_all.wait_send()
    dn_all.wait_send()
    for c in range(outer):
        @pl.when((c <= o) & (o + 1 < outer))
        def _():
            whole(nb.at[c, tp], zs.at[c, 1], zs.at[c, 1]).wait_send()

        @pl.when((c >= o) & (o > 0))
        def _():
            whole(nb.at[c, tp], zs.at[c, 0], zs.at[c, 0]).wait_send()

    whole(s1.at[:, pl.ds(0, hi - 1)], hs, hs).wait_send()
    whole(s1, ls, ls).wait_send()
    whole(s1, q1s, q1s).wait_send()
    whole(s2, q2s, q2s).wait_send()
    whole(s3.at[:, pl.ds(0, outer - 1)], q3s, q3s).wait_send()


def on_device(
    sp_size, tp_size, query, forget_logits, written_values, output_gate_logits, forget_floor_gap,
    extra_log_decay, head_norm_gain, output_weight, residual, mixer_norm_gain, mixer_up_weight,
    mixer_down_weight,
):
    rows, depth = residual.shape
    length, local_width = query.shape
    heads = local_width // HEAD_K
    depth_part, cols = mixer_up_weight.shape
    down_rows = mixer_down_weight.shape[0]
    inner, hi = sp_size // OUTER, tp_size // LO
    width = cols // OUTER
    up_pieces = max(1, min(2, depth_part // 128))
    down_pieces = max(1, min(2, down_rows // 64))
    steps = len(doubling(sp_size))
    f32, b16 = jnp.float32, jnp.bfloat16
    dma = pltpu.SemaphoreType.DMA
    vm = pltpu.VMEM
    O, F, C, half = OUTER, pieces_of(rows), halves_of(rows), depth // 2
    lrows = 8 * ((heads + 7) // 8)
    return pl.pallas_call(
        functools.partial(layer_kernel, sp_size, tp_size, up_pieces, down_pieces),
        out_shape=jax.ShapeDtypeStruct((rows, depth), b16),
        in_specs=[pl.BlockSpec(memory_space=pltpu.HBM)] * 12,
        out_specs=pl.BlockSpec(memory_space=pltpu.VMEM),
        scratch_shapes=[
            vm((length, local_width), b16), vm((length, local_width), b16),
            vm((length, local_width), b16), vm((length, local_width), b16),
            vm((length, local_width), f32),
            vm((1, local_width), f32), vm((1, HEAD_V), f32), vm((1, depth), f32),
            vm((rows, depth), b16),
            vm((length, local_width), f32), vm((length, local_width), f32),
            vm((length, local_width), f32), vm((length, local_width), b16),
            vm((heads, HEAD_V, HEAD_K), f32), vm((lrows, HEAD_K), f32),
            vm((heads, HEAD_V, HEAD_K), f32), vm((lrows, HEAD_K), f32),
            vm((steps, heads, HEAD_V, HEAD_K), b16), vm((steps, lrows, HEAD_K), f32),
            vm((steps, heads, HEAD_V, HEAD_K), b16), vm((steps, lrows, HEAD_K), f32),
            vm((tp_size, rows, local_width), b16), vm((LO, hi, rows, local_width), b16),
            vm((LO, local_width, depth), b16),
            vm((sp_size, depth_part, width), b16),
            vm((inner, down_rows, depth), b16),
            vm((hi, rows, depth), b16), vm((hi, rows, depth), b16),
            vm((rows, depth), f32),
            vm((O, tp_size, rows, depth), b16),
            vm((O, tp_size * rows, width), b16),
            vm((tp_size, rows, half), f32),
            vm((2 * O, hi, rows, half), f32),
            vm((2 * O, hi, rows, half), b16), vm((2 * O, hi, rows, half), b16),
            vm((2 * O, hi - 1, rows, half), b16), vm((2 * O, hi - 1, rows, half), b16),
            vm((2 * O, rows, half), f32),
            vm((2, O, rows, half), b16), vm((2, O + 1, rows, half), b16),
            dma((12,)),
            dma((steps,)), dma((steps,)), dma((steps,)), dma((steps,)),
            dma, dma, dma, dma,
            dma, dma((hi - 1, F)),
            dma, dma((O, up_pieces)),
            dma, dma, dma, dma((2,)),
            dma((O, 2)), dma((O, F)),
            dma, dma((O, hi - 1, F)),
            dma, dma((O,)),
            dma, dma((2 * O,)), dma, dma((2 * O, hi - 1, C)),
            dma, dma((2, O + 1, C)),
        ],
        compiler_params=pltpu.CompilerParams(
            collective_id=0, has_side_effects=True, vmem_limit_bytes=60 * 1024 * 1024
        ),
    )(
        query, forget_logits, written_values, output_gate_logits, forget_floor_gap.reshape(1, -1),
        extra_log_decay, head_norm_gain.reshape(1, -1), output_weight, residual,
        mixer_norm_gain.reshape(1, -1), mixer_up_weight, mixer_down_weight,
    )


def solution(mesh):
    return jax.shard_map(
        functools.partial(on_device, mesh.shape["sp"], mesh.shape["tp"]),
        mesh=mesh,
        in_specs=(
            P("sp", "tp"),
            P("sp", "tp"),
            P("sp", "tp"),
            P("sp", "tp"),
            P("tp"),
            P("sp", "tp"),
            P(),
            P("tp", None),
            P(("sp", "tp"), None),
            P(),
            P("sp", "tp"),
            P(("tp", "sp"), None),
        ),
        out_specs=P(("sp", "tp"), None),
        check_vma=False,
    )
```

```python
import functools

import jax
import jax.numpy as jnp
from jax import lax
from jax.experimental import pallas as pl
from jax.experimental.pallas import tpu as pltpu
from jax.sharding import PartitionSpec as P

HEAD_K = 128
HEAD_V = 128
CHUNK = 128
OUTER = 4
LO = 2
MESH = pl.DeviceIdType.MESH
norm_eps = 1e-06


def doubling(n):
    d, out = 1, []
    while d < n:
        out.append(d)
        d *= 2
    return out


def hops(n):
    return [s * k for k in range(1, n) for s in (1, -1)]


def pieces_of(rows):
    return max(1, rows // 16)


def halves_of(rows):
    return max(1, rows // 32)


def by_distance(n):
    return [
        sorted(range(n), key=lambda c: (abs(c - o), c if 2 * o < n else -c)) for o in range(n)
    ]


def dot_t(a, b):
    return lax.dot_general(a, b, (((1,), (1,)), ((), ())), preferred_element_type=jnp.float32)


def dot_0(a, b):
    return lax.dot_general(a, b, (((0,), (0,)), ((), ())), preferred_element_type=jnp.float32)


def dot(a, b):
    return jnp.dot(a, b, preferred_element_type=jnp.float32)


def layer_kernel(
    sp_size, tp_size, up_pieces, down_pieces,
    q_hbm, f_hbm, v_hbm, g_hbm, gap_hbm, ex_hbm, hg_hbm, wo_hbm, res_hbm, mg_hbm, up_hbm, dn_hbm,
    out_ref,
    qb, fb, vb, gb, exb, gapb, hgb, mgb, resb,
    cumb, gateb, recb, qcb, own, ownl, exc, excl, ss, sl, rs_, rl,
    mixb, mx, wob, upb, dnb, s6, r6,
    stream, nb, hid, pbuf, acc, s1, r1, s2, r2, acc2, s3, r3,
    ldsem, sts, str_, lts, ltr, mxs, mxr, wos, wor, q6s, q6r, us, ur, fs, fr, dsn, dr,
    zs, zr, hs, hr, ls, lr, q1s, q1r, q2s, q2r, q3s, q3r,
):
    outer, inner, hi = OUTER, sp_size // OUTER, tp_size // LO
    sp, tp = lax.axis_index("sp"), lax.axis_index("tp")
    o, i = lax.div(sp, inner), lax.rem(sp, inner)
    h, l = lax.div(tp, LO), lax.rem(tp, LO)
    other = 1 - l
    rows, depth = res_hbm.shape
    length, local_width = q_hbm.shape
    heads = local_width // HEAD_K
    depth_part, cols = up_hbm.shape
    width = cols // outer
    down_rows = dn_hbm.shape[0]
    f32, b16 = jnp.float32, jnp.bfloat16
    steps = doubling(sp_size)
    fine = pieces_of(rows)
    part_rows = rows // fine
    coarse = halves_of(rows)
    sum_rows = rows // coarse
    half = depth // 2

    def dev(ss_, tt):
        return (ss_, tt)

    def at_h(m):
        return lax.rem(h + m, hi)

    def from_h(m):
        return lax.rem(h - m + hi, hi)

    def at_i(m):
        return lax.rem(i + m, inner)

    def from_i(m):
        return lax.rem(i - m + inner, inner)

    def at_t(m):
        return lax.rem(tp + m, tp_size)

    def from_t(m):
        return lax.rem(tp - m + tp_size, tp_size)

    def rcopy(src, dst, ssem, rsem, device):
        return pltpu.make_async_remote_copy(
            src_ref=src, dst_ref=dst, send_sem=ssem, recv_sem=rsem,
            device_id=device, device_id_type=MESH,
        )

    loads = [
        pltpu.make_async_copy(src, dst, ldsem.at[n])
        for n, (src, dst) in enumerate(
            [
                (f_hbm, fb), (ex_hbm, exb), (gap_hbm, gapb), (v_hbm, vb), (q_hbm, qb), (g_hbm, gb),
                (hg_hbm, hgb), (mg_hbm, mgb), (res_hbm, resb),
                (wo_hbm, wob.at[l]),
                (up_hbm.at[:, pl.ds(pl.multiple_of(o * width, width), width)], upb.at[sp]),
                (dn_hbm, dnb.at[i]),
            ]
        )
    ]
    for c in loads:
        c.start()

    barrier = pltpu.get_barrier_semaphore()
    peers = [dev(lax.rem(o + k, outer) * inner + i, tp) for k in range(1, outer)]
    peers += [dev(o * inner + at_i(m), tp) for m in range(1, inner)]
    peers += [dev(sp, at_t(m)) for m in range(1, tp_size)]
    for d in steps:
        peers += [dev(lax.rem(sp + d, sp_size), tp), dev(lax.rem(sp - d + sp_size, sp_size), tp)]
    for peer in peers:
        pl.semaphore_signal(barrier, inc=1, device_id=peer, device_id_type=MESH)
    pl.semaphore_wait(barrier, len(peers))

    up_rows = depth_part // up_pieces
    dn_rows = down_rows // down_pieces

    def up_cols(to, p):
        return up_hbm.at[
            pl.ds(p * up_rows, up_rows), pl.ds(pl.multiple_of(to * width, width), width)
        ]

    def up_place(source, p):
        return upb.at[source, pl.ds(p * up_rows, up_rows)]

    def up_send(to, p):
        return rcopy(
            up_cols(to, p), up_place(sp, p), us, ur.at[o, p], dev(to * inner + i, tp)
        )

    def up_recv(source, p):
        place = up_place(source * inner + i, p)
        return rcopy(place, place, us, ur.at[source, p], dev(source * inner + i, tp))

    def fw_send(source, p, m, src):
        return rcopy(
            src, up_place(source * inner + i, p), fs, fr,
            dev(o * inner + at_i(m), tp),
        )

    def dn_send(n, p, m):
        part, at = pl.ds(p * dn_rows, dn_rows), pl.ds(n * half, half)
        return rcopy(
            dn_hbm.at[part, at], dnb.at[i, part, at], dsn, dr.at[n], dev(o * inner + at_i(m), tp)
        )

    def whole(ref, ssem, rsem):
        return rcopy(ref, ref, ssem, rsem, dev(sp, at_t(1)))

    fw_all = whole(upb.at[pl.ds(0, outer * (inner - 1))], fs, fr)
    dn_all = whole(dnb.at[pl.ds(0, inner - 1)], dsn, dsn)

    def dn_half(n):
        return whole(dnb.at[pl.ds(0, inner - 1), :, pl.ds(n * half, half)], dsn, dr.at[n])

    up_all = whole(upb.at[pl.ds(0, outer - 1)], us, us)

    def inside(k):
        return (o + k >= 0) & (o + k < outer)

    def up_issue(items):
        for k, p in items:
            @pl.when(inside(k))
            def _():
                up_send(o + k, p).start()

    def own_issue(p):
        for m in range(1, inner):
            fw_send(o, p, m, up_cols(o, p)).start()

    def dn_issue(items):
        for n, p in items:
            for m in range(1, inner):
                dn_send(n, p, m).start()

    dn_list = [(n, p) for n in range(2) for p in range(down_pieces)]

    def fw_issue(items):
        for k, p in items:
            @pl.when(inside(k))
            def _():
                up_recv(o + k, p).wait_recv()
                for m in range(1, inner):
                    fw_send(o + k, p, m, up_place((o + k) * inner + i, p)).start()

    up_list = [(k, p) for k in hops(outer)[::-1] for p in range(up_pieces)]
    near = [(k, p) for k, p in up_list if abs(k) == 1]
    far = [(k, p) for k, p in up_list if abs(k) > 1]
    falling = [(k, p) for k, p in up_list if k < 0]
    rising = [(k, p) for k, p in near if k > 0]
    rising_far = [(k, p) for k, p in far if k > 0]

    def piece(q):
        return pl.ds(q * part_rows, part_rows)

    def wo_copy():
        return rcopy(wo_hbm, wob.at[l], wos, wor, dev(sp, h * LO + other))

    wo_copy().start()
    up_issue(falling)
    for c in loads[:4]:
        c.wait()
    gate = gapb[...] / (1.0 + jnp.exp(fb[...].astype(f32)))
    gateb[...] = gate
    log_rate = jnp.log(1.0 - gate) + exb[...]
    top = log_rate.astype(b16)
    left = log_rate - top.astype(f32)
    middle = left.astype(b16)
    low = (left - middle.astype(f32)).astype(b16)
    causal = lax.broadcasted_iota(jnp.int32, (length, length), 0) >= lax.broadcasted_iota(
        jnp.int32, (length, length), 1
    )
    ones = jnp.where(causal, 1.0, 0.0).astype(b16)
    cum = dot(ones, top) + (dot(ones, middle) + dot(ones, low))
    cumb[...] = cum
    total_log = cum[length - 1 : length, :]
    written = (gate * jnp.exp(total_log - cum)).astype(b16)
    exc[...] = jnp.zeros_like(exc)
    excl[...] = jnp.zeros_like(excl)
    sl[...] = jnp.zeros_like(sl)
    for n in range(heads):
        at = slice(n * HEAD_K, (n + 1) * HEAD_K)
        state = dot_0(vb[:, at], written[:, at])
        own[n] = state
        ss[0, n] = state.astype(b16)
        ownl[n : n + 1, :] = total_log[:, at]
        sl[0, n : n + 1, :] = total_log[:, at]

    def st_send(n):
        return rcopy(ss.at[n], rs_.at[n], sts.at[n], str_.at[n], dev(sp + steps[n], tp))

    def lt_send(n):
        return rcopy(sl.at[n], rl.at[n], lts.at[n], ltr.at[n], dev(sp + steps[n], tp))

    def step_send(n):
        @pl.when(sp + steps[n] < sp_size)
        def _():
            lt_send(n).start()
            st_send(n).start()

    def step_recv(n):
        @pl.when(sp >= steps[n])
        def _():
            lt_send(n).wait_recv()
            st_send(n).wait_recv()
            for k in range(heads):
                exc[k] = exc[k] + jnp.exp(excl[k : k + 1, :]) * rs_[n, k].astype(f32)
                excl[k : k + 1, :] = excl[k : k + 1, :] + rl[n, k : k + 1, :]

    def step_pack(n):
        for k in range(heads):
            ss[n, k] = (own[k] + jnp.exp(ownl[k : k + 1, :]) * exc[k]).astype(b16)
            sl[n, k : k + 1, :] = ownl[k : k + 1, :] + excl[k : k + 1, :]

    step_send(0)
    up_issue(rising[:1])
    for p in range(up_pieces):
        own_issue(p)
    dn_issue(dn_list[:-1])

    loads[4].wait()
    scaled = qb[...].astype(f32) * HEAD_K ** (-0.5)
    qcb[...] = (scaled * jnp.exp(cum)).astype(b16)
    blocks = length // CHUNK
    tri = causal[:CHUNK, :CHUNK]
    for a in range(blocks):
        r = slice(a * CHUNK, (a + 1) * CHUNK)
        c_a, g_a, q_a = cum[r], gate[r], scaled[r]
        end = cum[(a + 1) * CHUNK - 1 : (a + 1) * CHUNK, :]
        base = cum[a * CHUNK - 1 : a * CHUNK, :] if a else jnp.zeros_like(end)
        mid = 0.5 * (end + base)
        q_d = (q_a * jnp.exp(c_a - mid)).astype(b16)
        k_d = (g_a * jnp.exp(mid - c_a)).astype(b16)
        if a:
            before = slice(0, a * CHUNK)
            q_o = (q_a * jnp.exp(c_a - base)).astype(b16)
            k_o = (gate[before] * jnp.exp(base - cum[before])).astype(b16)
        for n in range(heads):
            at = slice(n * HEAD_K, (n + 1) * HEAD_K)
            score = jnp.where(tri, dot_t(q_d[:, at], k_d[:, at]), 0.0).astype(b16)
            got = dot(score, vb[r, at])
            if a:
                score = dot_t(q_o[:, at], k_o[:, at]).astype(b16)
                got = got + dot(score, vb[before, at])
            recb[r, at] = got

    for n in range(len(steps)):
        step_recv(n)
        if n + 1 < len(steps):
            step_pack(n + 1)
            step_send(n + 1)
            if n == 0:
                up_issue(rising[1:])
            if n + 2 == len(steps):
                @pl.when(o > 0)
                def _():
                    up_issue(rising_far)
    if len(steps) < 2:
        up_issue(rising[1:])

        @pl.when(o > 0)
        def _():
            up_issue(rising_far)

    loads[5].wait()
    loads[6].wait()
    for n in range(heads):
        at = slice(n * HEAD_K, (n + 1) * HEAD_K)
        rec = recb[:, at] + dot_t(qcb[:, at], exc[n].astype(b16))
        logits = gb[:, at].astype(f32)
        normal = rec * lax.rsqrt(jnp.mean(rec * rec, axis=-1, keepdims=True) + norm_eps)
        mixed = (normal * hgb[...] * (logits / (1.0 + jnp.exp(-logits)))).astype(b16)
        mixb[:, :, at] = mixed.reshape(tp_size, rows, HEAD_V)

    def mx_copy(hh):
        return rcopy(
            mixb.at[hh * LO + other], mx.at[l, hh], mxs, mxr, dev(sp, h * LO + other)
        )

    def p6_copy(m, q):
        return rcopy(
            s6.at[m, piece(q)], r6.at[m, piece(q)], q6s, q6r.at[m - 1, q],
            dev(sp, at_h(m) * LO + l),
        )

    for hh in range(hi):
        mx_copy(hh).start()
    for hh in range(hi):
        mx[l, hh] = mixb[hh * LO + l]
    for c in loads[7:10]:
        c.wait()
    wo_copy().wait_recv()
    mx_all = whole(mx.at[0], mxs, mxr)
    mx_all.wait_recv()

    def projected(hh):
        got = dot(mx[0, hh], wob[0])
        for ll in range(1, LO):
            got = got + dot(mx[ll, hh], wob[ll])
        return got

    for m in range(1, hi):
        s6[m] = projected(at_h(m)).astype(b16)
        for q in range(fine):
            p6_copy(m, q).start()
    stream[...] = resb[...].astype(f32) + projected(h)

    table = by_distance(outer)

    def chunk_at(p):
        c = 0
        for oo in range(outer):
            for pp in range(outer):
                c = jnp.where((o == oo) & (p == pp), table[oo][pp], c)
        return c

    def z_copy(c, q, to):
        ref = nb.at[c, tp, piece(q)]
        return rcopy(ref, ref, zs.at[c, jnp.where(to > o, 1, 0)], zr.at[c, q], dev(to * inner + i, tp))

    def h_copy(c, q, m):
        ref = nb.at[c, tp, piece(q)]
        return rcopy(ref, ref, hs, hr.at[c, m - 1, q], dev(sp, at_h(m) * LO + l))

    def l_copy(c, q):
        ref = nb.at[c, tp, piece(q)]
        return rcopy(ref, ref, ls, lr.at[c], dev(sp, h * LO + other))

    def l2_copy(c, q, m):
        ref = nb.at[c, from_h(m) * LO + l, piece(q)]
        return rcopy(ref, ref, ls, lr.at[c], dev(sp, h * LO + other))

    def pass_on(c, q):
        @pl.when((c <= o) & (o + 1 < outer))
        def _():
            z_copy(c, q, o + 1).start()

        @pl.when((c >= o) & (o > 0))
        def _():
            z_copy(c, q, o - 1).start()

    def spread(c, q):
        for m in range(1, hi):
            h_copy(c, q, m).start()
        l_copy(c, q).start()

    def gather(c, q):
        for m in range(1, hi):
            h_copy(c, q, m).wait_recv()
            l2_copy(c, q, m).start()

    for q in range(fine):
        r = slice(q * part_rows, (q + 1) * part_rows)
        total = stream[r]
        for m in range(1, hi):
            p6_copy(m, q).wait_recv()
            total = total + r6[m, r].astype(f32)
        stream[r] = total
        scale = lax.rsqrt(jnp.mean(total * total, axis=-1, keepdims=True) + norm_eps)
        nb[o, tp, r] = (total * scale * mgb[...]).astype(b16)
        pass_on(o, q)
        spread(o, q)

    @pl.when(o == 0)
    def _():
        up_issue(rising_far)

    for p in range(1, outer):
        c = chunk_at(p)
        for q in range(fine):
            z_copy(c, q, o).wait_recv()
            pass_on(c, q)
            spread(c, q)
            gather(chunk_at(p - 1), q)
            if p == 1 and q == 0:
                fw_issue(near)
            if p == 1 and q == fine // 2:
                fw_issue([it for it in far if it[0] > 0])
        if p == 1:
            fw_issue([it for it in far if it[0] < 0])
            dn_issue(dn_list[-1:])
    def gather_last():
        for q in range(fine):
            gather(chunk_at(outer - 1), q)

    @pl.when(o + 1 < outer)
    def _():
        gather_last()

    for c in loads[10:]:
        c.wait()
    fw_all.wait_recv()
    dn_half(0).wait_recv()

    def s1_copy(k):
        return rcopy(s1.at[k], r1.at[k], q1s, q1r.at[k], dev(sp, h * LO + other))

    def rows_of(q):
        return slice(q * sum_rows, (q + 1) * sum_rows)

    def s2_copy(k, m, q):
        r = pl.ds(q * sum_rows, sum_rows)
        return rcopy(
            s2.at[k, m - 1, r], r2.at[k, m - 1, r], q2s, q2r.at[k, m - 1, q],
            dev(sp, at_h(m) * LO + l),
        )

    def before(c):
        return jnp.where(c > o, o > 0, o + 1 < outer)

    def s3_copy(n, c, q):
        to = jnp.where(c > o, o + 1, o - 1)
        slot = jnp.where((c < o) & (c == to), outer, c)
        r = pl.ds(q * sum_rows, sum_rows)
        return rcopy(
            s3.at[n, c, r], r3.at[n, slot, r], q3s, q3r.at[n, slot, q], dev(to * inner + i, tp)
        )

    def s3_recv(n, slot, q):
        place = r3.at[n, slot, pl.ds(q * sum_rows, sum_rows)]
        return rcopy(place, place, q3s, q3r.at[n, slot, q], dev(sp, at_t(1)))

    def relay(k, q):
        n, c, r = half_of(k), turn(k), rows_of(q)

        @pl.when(before(c))
        def _():
            s3_recv(n, c, q).wait_recv()
            acc2[k, r] = acc2[k, r] + r3[n, c, r].astype(f32)

        s3[n, c, r] = acc2[k, r].astype(b16)
        s3_copy(n, c, q).start()

    slots, lag = 2 * outer, 3

    def turn(j):
        p = jnp.where((j == 0) | (j == slots - 3), 1, outer - 1 - (j - 1) // 2)
        return chunk_at(jnp.where(j >= slots - 2, 0, p))

    def half_of(j):
        return jnp.where(j >= slots - 3, jnp.where(j == slots - 2, 0, 1), jnp.where(j == 0, 0, lax.rem(j + 1, 2)))

    def send_sums(k):
        s1_copy(k).wait_recv()
        for m in range(1, hi):
            to = at_h(m)
            for q in range(coarse):
                r = rows_of(q)
                s2[k, m - 1, r] = (acc[k, to, r] + r1[k, to, r].astype(f32)).astype(b16)
                s2_copy(k, m, q).start()
        acc2[k] = acc[k, h] + r1[k, h].astype(f32)

    def collect(k):
        for q in range(coarse):
            r = rows_of(q)
            v = acc2[k, r]
            for m in range(1, hi):
                s2_copy(k, m, q).wait_recv()
                v = v + r2[k, m - 1, r].astype(f32)
            acc2[k, r] = v

            @pl.when((k < slots - 2) & jnp.logical_not(before(turn(k))))
            def _():
                relay(k, q)

            @pl.when((k == slots - 3) & before(turn(0)))
            def _():
                relay(0, q)

            @pl.when((k >= 2) & (k < slots - 1) & before(turn(k - 1)))
            def _():
                relay(k - 1, q)

    def body(j, carry):
        @pl.when(j == 1)
        def _():
            send_sums(0)
            @pl.when(o + 1 == outer)
            def _():
                gather_last()

        @pl.when(j < slots)
        def _():
            c = turn(j)

            @pl.when((j == 0) | (j == slots - 2) | ((j < slots - 3) & (lax.rem(j, 2) == 1)))
            def _():
                whole(nb.at[c, pl.ds(0, hi)], ls, lr.at[c]).wait_recv()
                x = nb[c].reshape(tp_size * rows, depth)
                lifted = dot(x, upb[...].reshape(depth, width))
                hid[c] = jnp.square(jnp.maximum(lifted, 0.0)).astype(b16)

            @pl.when(j == 2)
            def _():
                dn_half(1).wait_recv()

            at = pl.ds(pl.multiple_of(half_of(j) * half, half), half)
            part = dot(hid[c], dnb[:, :, at].reshape(width, half))
            pbuf[...] = part.reshape(tp_size, rows, half)
            for hh in range(hi):
                s1[j, hh] = pbuf[hh * LO + other].astype(b16)
            s1_copy(j).start()
            for hh in range(hi):
                acc[j, hh] = pbuf[hh * LO + l]

        @pl.when((j >= 2) & (j < slots + 1))
        def _():
            send_sums(j - 1)

        @pl.when(j >= lag)
        def _():
            collect(j - lag)

        return carry

    lax.fori_loop(0, slots + lag, body, 0)

    for n in range(2):
        at = slice(n * half, (n + 1) * half)
        mine = slots - 2 + n
        for q in range(coarse):
            r = rows_of(q)

            @pl.when(o > 0)
            def _():
                s3_recv(n, o, q).wait_recv()
                acc2[mine, r] = acc2[mine, r] + r3[n, o, r].astype(f32)

            @pl.when(o + 1 < outer)
            def _():
                s3_recv(n, outer, q).wait_recv()
                acc2[mine, r] = acc2[mine, r] + r3[n, outer, r].astype(f32)

            out_ref[r, at] = (stream[r, at] + acc2[mine, r]).astype(b16)

    wo_copy().wait_send()
    mx_all.wait_send()
    whole(s6.at[pl.ds(0, hi - 1)], q6s, q6s).wait_send()
    for n in range(len(steps)):
        @pl.when(sp + steps[n] < sp_size)
        def _():
            lt_send(n).wait_send()
            st_send(n).wait_send()
    up_all.wait_send()
    fw_all.wait_send()
    dn_all.wait_send()
    for c in range(outer):
        @pl.when((c <= o) & (o + 1 < outer))
        def _():
            whole(nb.at[c, tp], zs.at[c, 1], zs.at[c, 1]).wait_send()

        @pl.when((c >= o) & (o > 0))
        def _():
            whole(nb.at[c, tp], zs.at[c, 0], zs.at[c, 0]).wait_send()

    whole(s1.at[:, pl.ds(0, hi - 1)], hs, hs).wait_send()
    whole(s1, ls, ls).wait_send()
    whole(s1, q1s, q1s).wait_send()
    whole(s2, q2s, q2s).wait_send()
    whole(s3.at[:, pl.ds(0, outer - 1)], q3s, q3s).wait_send()


def on_device(
    sp_size, tp_size, query, forget_logits, written_values, output_gate_logits, forget_floor_gap,
    extra_log_decay, head_norm_gain, output_weight, residual, mixer_norm_gain, mixer_up_weight,
    mixer_down_weight,
):
    rows, depth = residual.shape
    length, local_width = query.shape
    heads = local_width // HEAD_K
    depth_part, cols = mixer_up_weight.shape
    down_rows = mixer_down_weight.shape[0]
    inner, hi = sp_size // OUTER, tp_size // LO
    width = cols // OUTER
    up_pieces = max(1, min(2, depth_part // 128))
    down_pieces = max(1, min(2, down_rows // 64))
    steps = len(doubling(sp_size))
    f32, b16 = jnp.float32, jnp.bfloat16
    dma = pltpu.SemaphoreType.DMA
    vm = pltpu.VMEM
    O, F, C, half = OUTER, pieces_of(rows), halves_of(rows), depth // 2
    lrows = 8 * ((heads + 7) // 8)
    return pl.pallas_call(
        functools.partial(layer_kernel, sp_size, tp_size, up_pieces, down_pieces),
        out_shape=jax.ShapeDtypeStruct((rows, depth), b16),
        in_specs=[pl.BlockSpec(memory_space=pltpu.HBM)] * 12,
        out_specs=pl.BlockSpec(memory_space=pltpu.VMEM),
        scratch_shapes=[
            vm((length, local_width), b16), vm((length, local_width), b16),
            vm((length, local_width), b16), vm((length, local_width), b16),
            vm((length, local_width), f32),
            vm((1, local_width), f32), vm((1, HEAD_V), f32), vm((1, depth), f32),
            vm((rows, depth), b16),
            vm((length, local_width), f32), vm((length, local_width), f32),
            vm((length, local_width), f32), vm((length, local_width), b16),
            vm((heads, HEAD_V, HEAD_K), f32), vm((lrows, HEAD_K), f32),
            vm((heads, HEAD_V, HEAD_K), f32), vm((lrows, HEAD_K), f32),
            vm((steps, heads, HEAD_V, HEAD_K), b16), vm((steps, lrows, HEAD_K), f32),
            vm((steps, heads, HEAD_V, HEAD_K), b16), vm((steps, lrows, HEAD_K), f32),
            vm((tp_size, rows, local_width), b16), vm((LO, hi, rows, local_width), b16),
            vm((LO, local_width, depth), b16),
            vm((sp_size, depth_part, width), b16),
            vm((inner, down_rows, depth), b16),
            vm((hi, rows, depth), b16), vm((hi, rows, depth), b16),
            vm((rows, depth), f32),
            vm((O, tp_size, rows, depth), b16),
            vm((O, tp_size * rows, width), b16),
            vm((tp_size, rows, half), f32),
            vm((2 * O, hi, rows, half), f32),
            vm((2 * O, hi, rows, half), b16), vm((2 * O, hi, rows, half), b16),
            vm((2 * O, hi - 1, rows, half), b16), vm((2 * O, hi - 1, rows, half), b16),
            vm((2 * O, rows, half), f32),
            vm((2, O, rows, half), b16), vm((2, O + 1, rows, half), b16),
            dma((12,)),
            dma((steps,)), dma((steps,)), dma((steps,)), dma((steps,)),
            dma, dma, dma, dma,
            dma, dma((hi - 1, F)),
            dma, dma((O, up_pieces)),
            dma, dma, dma, dma((2,)),
            dma((O, 2)), dma((O, F)),
            dma, dma((O, hi - 1, F)),
            dma, dma((O,)),
            dma, dma((2 * O,)), dma, dma((2 * O, hi - 1, C)),
            dma, dma((2, O + 1, C)),
        ],
        compiler_params=pltpu.CompilerParams(
            collective_id=0, has_side_effects=True, vmem_limit_bytes=60 * 1024 * 1024
        ),
    )(
        query, forget_logits, written_values, output_gate_logits, forget_floor_gap.reshape(1, -1),
        extra_log_decay, head_norm_gain.reshape(1, -1), output_weight, residual,
        mixer_norm_gain.reshape(1, -1), mixer_up_weight, mixer_down_weight,
    )


def solution(mesh):
    return jax.shard_map(
        functools.partial(on_device, mesh.shape["sp"], mesh.shape["tp"]),
        mesh=mesh,
        in_specs=(
            P("sp", "tp"),
            P("sp", "tp"),
            P("sp", "tp"),
            P("sp", "tp"),
            P("tp"),
            P("sp", "tp"),
            P(),
            P("tp", None),
            P(("sp", "tp"), None),
            P(),
            P("sp", "tp"),
            P(("tp", "sp"), None),
        ),
        out_specs=P(("sp", "tp"), None),
        check_vma=False,
    )
```

```python
import functools

import jax
import jax.numpy as jnp
from jax import lax
from jax.experimental import pallas as pl
from jax.experimental.pallas import tpu as pltpu
from jax.sharding import PartitionSpec as P

HEAD_K = 128
HEAD_V = 128
CHUNK = 128
OUTER = 4
LO = 2
MESH = pl.DeviceIdType.MESH
norm_eps = 1e-06


def doubling(n):
    d, out = 1, []
    while d < n:
        out.append(d)
        d *= 2
    return out


def hops(n):
    return [s * k for k in range(1, n) for s in (1, -1)]


def pieces_of(rows):
    return max(1, rows // 16)


def halves_of(rows):
    return max(1, rows // 32)


def by_distance(n):
    return [
        sorted(range(n), key=lambda c: (abs(c - o), c if 2 * o < n else -c)) for o in range(n)
    ]


def dot_t(a, b):
    return lax.dot_general(a, b, (((1,), (1,)), ((), ())), preferred_element_type=jnp.float32)


def dot_0(a, b):
    return lax.dot_general(a, b, (((0,), (0,)), ((), ())), preferred_element_type=jnp.float32)


def dot(a, b):
    return jnp.dot(a, b, preferred_element_type=jnp.float32)


def layer_kernel(
    sp_size, tp_size, up_pieces, down_pieces,
    q_hbm, f_hbm, v_hbm, g_hbm, gap_hbm, ex_hbm, hg_hbm, wo_hbm, res_hbm, mg_hbm, up_hbm, dn_hbm,
    out_ref,
    qb, fb, vb, gb, exb, gapb, hgb, mgb, resb,
    cumb, gateb, recb, qcb, own, ownl, exc, excl, ss, sl, rs_, rl,
    mixb, mx, wob, upb, dnb, s6, r6,
    stream, nb, hid, pbuf, acc, s1, r1, s2, r2, acc2, s3, r3,
    ldsem, sts, str_, lts, ltr, mxs, mxr, wos, wor, q6s, q6r, us, ur, fs, fr, dsn, dr,
    zs, zr, hs, hr, ls, lr, q1s, q1r, q2s, q2r, q3s, q3r,
):
    outer, inner, hi = OUTER, sp_size // OUTER, tp_size // LO
    sp, tp = lax.axis_index("sp"), lax.axis_index("tp")
    o, i = lax.div(sp, inner), lax.rem(sp, inner)
    h, l = lax.div(tp, LO), lax.rem(tp, LO)
    other = 1 - l
    rows, depth = res_hbm.shape
    length, local_width = q_hbm.shape
    heads = local_width // HEAD_K
    depth_part, cols = up_hbm.shape
    width = cols // outer
    down_rows = dn_hbm.shape[0]
    f32, b16 = jnp.float32, jnp.bfloat16
    steps = doubling(sp_size)
    fine = pieces_of(rows)
    part_rows = rows // fine
    coarse = halves_of(rows)
    sum_rows = rows // coarse
    half = depth // 2

    def dev(ss_, tt):
        return (ss_, tt)

    def at_h(m):
        return lax.rem(h + m, hi)

    def from_h(m):
        return lax.rem(h - m + hi, hi)

    def at_i(m):
        return lax.rem(i + m, inner)

    def from_i(m):
        return lax.rem(i - m + inner, inner)

    def at_t(m):
        return lax.rem(tp + m, tp_size)

    def from_t(m):
        return lax.rem(tp - m + tp_size, tp_size)

    def rcopy(src, dst, ssem, rsem, device):
        return pltpu.make_async_remote_copy(
            src_ref=src, dst_ref=dst, send_sem=ssem, recv_sem=rsem,
            device_id=device, device_id_type=MESH,
        )

    loads = [
        pltpu.make_async_copy(src, dst, ldsem.at[n])
        for n, (src, dst) in enumerate(
            [
                (f_hbm, fb), (ex_hbm, exb), (gap_hbm, gapb), (v_hbm, vb), (q_hbm, qb), (g_hbm, gb),
                (hg_hbm, hgb), (mg_hbm, mgb), (res_hbm, resb),
                (wo_hbm, wob.at[l]),
                (up_hbm.at[:, pl.ds(pl.multiple_of(o * width, width), width)], upb.at[sp]),
                (dn_hbm, dnb.at[i]),
            ]
        )
    ]
    for c in loads:
        c.start()

    barrier = pltpu.get_barrier_semaphore()
    peers = [dev(lax.rem(o + k, outer) * inner + i, tp) for k in range(1, outer)]
    peers += [dev(o * inner + at_i(m), tp) for m in range(1, inner)]
    peers += [dev(sp, at_t(m)) for m in range(1, tp_size)]
    for d in steps:
        peers += [dev(lax.rem(sp + d, sp_size), tp), dev(lax.rem(sp - d + sp_size, sp_size), tp)]
    for peer in peers:
        pl.semaphore_signal(barrier, inc=1, device_id=peer, device_id_type=MESH)
    pl.semaphore_wait(barrier, len(peers))

    up_rows = depth_part // up_pieces
    dn_rows = down_rows // down_pieces

    def up_cols(to, p):
        return up_hbm.at[
            pl.ds(p * up_rows, up_rows), pl.ds(pl.multiple_of(to * width, width), width)
        ]

    def up_place(source, p):
        return upb.at[source, pl.ds(p * up_rows, up_rows)]

    def up_send(to, p):
        return rcopy(
            up_cols(to, p), up_place(sp, p), us, ur.at[o, p], dev(to * inner + i, tp)
        )

    def up_recv(source, p):
        place = up_place(source * inner + i, p)
        return rcopy(place, place, us, ur.at[source, p], dev(source * inner + i, tp))

    def fw_send(source, p, m, src):
        return rcopy(
            src, up_place(source * inner + i, p), fs, fr,
            dev(o * inner + at_i(m), tp),
        )

    def dn_send(n, p, m):
        part, at = pl.ds(p * dn_rows, dn_rows), pl.ds(n * half, half)
        return rcopy(
            dn_hbm.at[part, at], dnb.at[i, part, at], dsn, dr.at[n], dev(o * inner + at_i(m), tp)
        )

    def whole(ref, ssem, rsem):
        return rcopy(ref, ref, ssem, rsem, dev(sp, at_t(1)))

    fw_all = whole(upb.at[pl.ds(0, outer * (inner - 1))], fs, fr)
    dn_all = whole(dnb.at[pl.ds(0, inner - 1)], dsn, dsn)

    def dn_half(n):
        return whole(dnb.at[pl.ds(0, inner - 1), :, pl.ds(n * half, half)], dsn, dr.at[n])

    up_all = whole(upb.at[pl.ds(0, outer - 1)], us, us)

    def inside(k):
        return (o + k >= 0) & (o + k < outer)

    def up_issue(items):
        for k, p in items:
            @pl.when(inside(k))
            def _():
                up_send(o + k, p).start()

    def own_issue(p):
        for m in range(1, inner):
            fw_send(o, p, m, up_cols(o, p)).start()

    def dn_issue(items):
        for n, p in items:
            for m in range(1, inner):
                dn_send(n, p, m).start()

    dn_list = [(n, p) for n in range(2) for p in range(down_pieces)]

    def fw_issue(items):
        for k, p in items:
            @pl.when(inside(k))
            def _():
                up_recv(o + k, p).wait_recv()
                for m in range(1, inner):
                    fw_send(o + k, p, m, up_place((o + k) * inner + i, p)).start()

    up_list = [(k, p) for k in hops(outer)[::-1] for p in range(up_pieces)]
    near = [(k, p) for k, p in up_list if abs(k) == 1]
    far = [(k, p) for k, p in up_list if abs(k) > 1]
    falling = [(k, p) for k, p in up_list if k < 0]
    rising = [(k, p) for k, p in near if k > 0]
    rising_far = [(k, p) for k, p in far if k > 0]

    def piece(q):
        return pl.ds(q * part_rows, part_rows)

    def wo_copy():
        return rcopy(wo_hbm, wob.at[l], wos, wor, dev(sp, h * LO + other))

    wo_copy().start()
    up_issue(falling)
    for c in loads[:4]:
        c.wait()
    gate = gapb[...] / (1.0 + jnp.exp(fb[...].astype(f32)))
    gateb[...] = gate
    log_rate = jnp.log(1.0 - gate) + exb[...]
    top = log_rate.astype(b16)
    left = log_rate - top.astype(f32)
    middle = left.astype(b16)
    low = (left - middle.astype(f32)).astype(b16)
    causal = lax.broadcasted_iota(jnp.int32, (length, length), 0) >= lax.broadcasted_iota(
        jnp.int32, (length, length), 1
    )
    ones = jnp.where(causal, 1.0, 0.0).astype(b16)
    cum = dot(ones, top) + (dot(ones, middle) + dot(ones, low))
    cumb[...] = cum
    total_log = cum[length - 1 : length, :]
    written = (gate * jnp.exp(total_log - cum)).astype(b16)
    exc[...] = jnp.zeros_like(exc)
    excl[...] = jnp.zeros_like(excl)
    sl[...] = jnp.zeros_like(sl)
    for n in range(heads):
        at = slice(n * HEAD_K, (n + 1) * HEAD_K)
        state = dot_0(vb[:, at], written[:, at])
        own[n] = state
        ss[0, n] = state.astype(b16)
        ownl[n : n + 1, :] = total_log[:, at]
        sl[0, n : n + 1, :] = total_log[:, at]

    def st_send(n):
        return rcopy(ss.at[n], rs_.at[n], sts.at[n], str_.at[n], dev(sp + steps[n], tp))

    def lt_send(n):
        return rcopy(sl.at[n], rl.at[n], lts.at[n], ltr.at[n], dev(sp + steps[n], tp))

    def step_send(n):
        @pl.when(sp + steps[n] < sp_size)
        def _():
            lt_send(n).start()
            st_send(n).start()

    def step_recv(n):
        @pl.when(sp >= steps[n])
        def _():
            lt_send(n).wait_recv()
            st_send(n).wait_recv()
            for k in range(heads):
                exc[k] = exc[k] + jnp.exp(excl[k : k + 1, :]) * rs_[n, k].astype(f32)
                excl[k : k + 1, :] = excl[k : k + 1, :] + rl[n, k : k + 1, :]

    def step_pack(n):
        for k in range(heads):
            ss[n, k] = (own[k] + jnp.exp(ownl[k : k + 1, :]) * exc[k]).astype(b16)
            sl[n, k : k + 1, :] = ownl[k : k + 1, :] + excl[k : k + 1, :]

    step_send(0)
    up_issue(rising[:1])
    for p in range(up_pieces):
        own_issue(p)
    dn_issue(dn_list[:-1])

    loads[4].wait()
    scaled = qb[...].astype(f32) * HEAD_K ** (-0.5)
    qcb[...] = (scaled * jnp.exp(cum)).astype(b16)
    blocks = length // CHUNK
    tri = causal[:CHUNK, :CHUNK]
    for a in range(blocks):
        r = slice(a * CHUNK, (a + 1) * CHUNK)
        c_a, g_a, q_a = cum[r], gate[r], scaled[r]
        end = cum[(a + 1) * CHUNK - 1 : (a + 1) * CHUNK, :]
        base = cum[a * CHUNK - 1 : a * CHUNK, :] if a else jnp.zeros_like(end)
        mid = 0.5 * (end + base)
        q_d = (q_a * jnp.exp(c_a - mid)).astype(b16)
        k_d = (g_a * jnp.exp(mid - c_a)).astype(b16)
        if a:
            before = slice(0, a * CHUNK)
            q_o = (q_a * jnp.exp(c_a - base)).astype(b16)
            k_o = (gate[before] * jnp.exp(base - cum[before])).astype(b16)
        for n in range(heads):
            at = slice(n * HEAD_K, (n + 1) * HEAD_K)
            score = jnp.where(tri, dot_t(q_d[:, at], k_d[:, at]), 0.0).astype(b16)
            got = dot(score, vb[r, at])
            if a:
                score = dot_t(q_o[:, at], k_o[:, at]).astype(b16)
                got = got + dot(score, vb[before, at])
            recb[r, at] = got

    for n in range(len(steps)):
        step_recv(n)
        if n + 1 < len(steps):
            step_pack(n + 1)
            step_send(n + 1)
            if n == 0:
                up_issue(rising[1:])
            if n + 2 == len(steps):
                @pl.when(o > 0)
                def _():
                    up_issue(rising_far)
    if len(steps) < 2:
        up_issue(rising[1:])

        @pl.when(o > 0)
        def _():
            up_issue(rising_far)

    loads[5].wait()
    loads[6].wait()
    for n in range(heads):
        at = slice(n * HEAD_K, (n + 1) * HEAD_K)
        rec = recb[:, at] + dot_t(qcb[:, at], exc[n].astype(b16))
        logits = gb[:, at].astype(f32)
        normal = rec * lax.rsqrt(jnp.mean(rec * rec, axis=-1, keepdims=True) + norm_eps)
        mixed = (normal * hgb[...] * (logits / (1.0 + jnp.exp(-logits)))).astype(b16)
        mixb[:, :, at] = mixed.reshape(tp_size, rows, HEAD_V)

    def mx_copy(hh):
        return rcopy(
            mixb.at[hh * LO + other], mx.at[l, hh], mxs, mxr, dev(sp, h * LO + other)
        )

    def p6_copy(m, q):
        return rcopy(
            s6.at[m, piece(q)], r6.at[m, piece(q)], q6s, q6r.at[m - 1, q],
            dev(sp, at_h(m) * LO + l),
        )

    for hh in range(hi):
        mx_copy(hh).start()
    for hh in range(hi):
        mx[l, hh] = mixb[hh * LO + l]
    for c in loads[7:10]:
        c.wait()
    wo_copy().wait_recv()
    mx_all = whole(mx.at[0], mxs, mxr)
    mx_all.wait_recv()

    def projected(hh):
        got = dot(mx[0, hh], wob[0])
        for ll in range(1, LO):
            got = got + dot(mx[ll, hh], wob[ll])
        return got

    for m in range(1, hi):
        s6[m] = projected(at_h(m)).astype(b16)
        for q in range(fine):
            p6_copy(m, q).start()
    stream[...] = resb[...].astype(f32) + projected(h)

    table = by_distance(outer)

    def chunk_at(p):
        c = 0
        for oo in range(outer):
            for pp in range(outer):
                c = jnp.where((o == oo) & (p == pp), table[oo][pp], c)
        return c

    def z_copy(c, q, to):
        ref = nb.at[c, tp, piece(q)]
        return rcopy(ref, ref, zs.at[c, jnp.where(to > o, 1, 0)], zr.at[c, q], dev(to * inner + i, tp))

    def h_copy(c, q, m):
        ref = nb.at[c, tp, piece(q)]
        return rcopy(ref, ref, hs, hr.at[c, m - 1, q], dev(sp, at_h(m) * LO + l))

    def l_copy(c, q):
        ref = nb.at[c, tp, piece(q)]
        return rcopy(ref, ref, ls, lr.at[c], dev(sp, h * LO + other))

    def l2_copy(c, q, m):
        ref = nb.at[c, from_h(m) * LO + l, piece(q)]
        return rcopy(ref, ref, ls, lr.at[c], dev(sp, h * LO + other))

    def pass_on(c, q):
        @pl.when((c <= o) & (o + 1 < outer))
        def _():
            z_copy(c, q, o + 1).start()

        @pl.when((c >= o) & (o > 0))
        def _():
            z_copy(c, q, o - 1).start()

    def spread(c, q):
        for m in range(1, hi):
            h_copy(c, q, m).start()
        l_copy(c, q).start()

    def gather(c, q):
        for m in range(1, hi):
            h_copy(c, q, m).wait_recv()
            l2_copy(c, q, m).start()

    for q in range(fine):
        r = slice(q * part_rows, (q + 1) * part_rows)
        total = stream[r]
        for m in range(1, hi):
            p6_copy(m, q).wait_recv()
            total = total + r6[m, r].astype(f32)
        stream[r] = total
        scale = lax.rsqrt(jnp.mean(total * total, axis=-1, keepdims=True) + norm_eps)
        nb[o, tp, r] = (total * scale * mgb[...]).astype(b16)
        pass_on(o, q)
        spread(o, q)

    @pl.when(o == 0)
    def _():
        up_issue(rising_far[:2])

    for p in range(1, outer):
        c = chunk_at(p)
        for q in range(fine):
            z_copy(c, q, o).wait_recv()
            pass_on(c, q)
            spread(c, q)
            gather(chunk_at(p - 1), q)
            if p == 1 and q == 0:
                @pl.when(o == 0)
                def _():
                    up_issue(rising_far[2:])

                fw_issue(near)
            if p == 1 and q == fine // 2:
                fw_issue([it for it in far if it[0] > 0])
        if p == 1:
            fw_issue([it for it in far if it[0] < 0])
            dn_issue(dn_list[-1:])
    def gather_last():
        for q in range(fine):
            gather(chunk_at(outer - 1), q)

    @pl.when(o + 1 < outer)
    def _():
        gather_last()

    for c in loads[10:]:
        c.wait()
    fw_all.wait_recv()
    dn_half(0).wait_recv()

    def s1_copy(k):
        return rcopy(s1.at[k], r1.at[k], q1s, q1r.at[k], dev(sp, h * LO + other))

    def rows_of(q):
        return slice(q * sum_rows, (q + 1) * sum_rows)

    def s2_copy(k, m, q):
        r = pl.ds(q * sum_rows, sum_rows)
        return rcopy(
            s2.at[k, m - 1, r], r2.at[k, m - 1, r], q2s, q2r.at[k, m - 1, q],
            dev(sp, at_h(m) * LO + l),
        )

    def before(c):
        return jnp.where(c > o, o > 0, o + 1 < outer)

    def s3_copy(n, c, q):
        to = jnp.where(c > o, o + 1, o - 1)
        slot = jnp.where((c < o) & (c == to), outer, c)
        r = pl.ds(q * sum_rows, sum_rows)
        return rcopy(
            s3.at[n, c, r], r3.at[n, slot, r], q3s, q3r.at[n, slot, q], dev(to * inner + i, tp)
        )

    def s3_recv(n, slot, q):
        place = r3.at[n, slot, pl.ds(q * sum_rows, sum_rows)]
        return rcopy(place, place, q3s, q3r.at[n, slot, q], dev(sp, at_t(1)))

    def relay(k, q):
        n, c, r = half_of(k), turn(k), rows_of(q)

        @pl.when(before(c))
        def _():
            s3_recv(n, c, q).wait_recv()
            acc2[k, r] = acc2[k, r] + r3[n, c, r].astype(f32)

        s3[n, c, r] = acc2[k, r].astype(b16)
        s3_copy(n, c, q).start()

    slots, lag = 2 * outer, 3

    def turn(j):
        p = jnp.where((j == 0) | (j == slots - 3), 1, outer - 1 - (j - 1) // 2)
        return chunk_at(jnp.where(j >= slots - 2, 0, p))

    def half_of(j):
        return jnp.where(j >= slots - 3, jnp.where(j == slots - 2, 0, 1), jnp.where(j == 0, 0, lax.rem(j + 1, 2)))

    def send_sums(k):
        s1_copy(k).wait_recv()
        for m in range(1, hi):
            to = at_h(m)
            for q in range(coarse):
                r = rows_of(q)
                s2[k, m - 1, r] = (acc[k, to, r] + r1[k, to, r].astype(f32)).astype(b16)
                s2_copy(k, m, q).start()
        acc2[k] = acc[k, h] + r1[k, h].astype(f32)

    def collect(k):
        for q in range(coarse):
            r = rows_of(q)
            v = acc2[k, r]
            for m in range(1, hi):
                s2_copy(k, m, q).wait_recv()
                v = v + r2[k, m - 1, r].astype(f32)
            acc2[k, r] = v

            @pl.when((k < slots - 2) & jnp.logical_not(before(turn(k))))
            def _():
                relay(k, q)

            @pl.when((k == slots - 3) & before(turn(0)))
            def _():
                relay(0, q)

            @pl.when((k >= 2) & (k < slots - 1) & before(turn(k - 1)))
            def _():
                relay(k - 1, q)

    def body(j, carry):
        @pl.when(j == 1)
        def _():
            send_sums(0)
            @pl.when(o + 1 == outer)
            def _():
                gather_last()

        @pl.when(j < slots)
        def _():
            c = turn(j)

            @pl.when((j == 0) | (j == slots - 2) | ((j < slots - 3) & (lax.rem(j, 2) == 1)))
            def _():
                whole(nb.at[c, pl.ds(0, hi)], ls, lr.at[c]).wait_recv()
                x = nb[c].reshape(tp_size * rows, depth)
                lifted = dot(x, upb[...].reshape(depth, width))
                hid[c] = jnp.square(jnp.maximum(lifted, 0.0)).astype(b16)

            @pl.when(j == 2)
            def _():
                dn_half(1).wait_recv()

            at = pl.ds(pl.multiple_of(half_of(j) * half, half), half)
            part = dot(hid[c], dnb[:, :, at].reshape(width, half))
            pbuf[...] = part.reshape(tp_size, rows, half)
            for hh in range(hi):
                s1[j, hh] = pbuf[hh * LO + other].astype(b16)
            s1_copy(j).start()
            for hh in range(hi):
                acc[j, hh] = pbuf[hh * LO + l]

        @pl.when((j >= 2) & (j < slots + 1))
        def _():
            send_sums(j - 1)

        @pl.when(j >= lag)
        def _():
            collect(j - lag)

        return carry

    lax.fori_loop(0, slots + lag, body, 0)

    for n in range(2):
        at = slice(n * half, (n + 1) * half)
        mine = slots - 2 + n
        for q in range(coarse):
            r = rows_of(q)

            @pl.when(o > 0)
            def _():
                s3_recv(n, o, q).wait_recv()
                acc2[mine, r] = acc2[mine, r] + r3[n, o, r].astype(f32)

            @pl.when(o + 1 < outer)
            def _():
                s3_recv(n, outer, q).wait_recv()
                acc2[mine, r] = acc2[mine, r] + r3[n, outer, r].astype(f32)

            out_ref[r, at] = (stream[r, at] + acc2[mine, r]).astype(b16)

    wo_copy().wait_send()
    mx_all.wait_send()
    whole(s6.at[pl.ds(0, hi - 1)], q6s, q6s).wait_send()
    for n in range(len(steps)):
        @pl.when(sp + steps[n] < sp_size)
        def _():
            lt_send(n).wait_send()
            st_send(n).wait_send()
    up_all.wait_send()
    fw_all.wait_send()
    dn_all.wait_send()
    for c in range(outer):
        @pl.when((c <= o) & (o + 1 < outer))
        def _():
            whole(nb.at[c, tp], zs.at[c, 1], zs.at[c, 1]).wait_send()

        @pl.when((c >= o) & (o > 0))
        def _():
            whole(nb.at[c, tp], zs.at[c, 0], zs.at[c, 0]).wait_send()

    whole(s1.at[:, pl.ds(0, hi - 1)], hs, hs).wait_send()
    whole(s1, ls, ls).wait_send()
    whole(s1, q1s, q1s).wait_send()
    whole(s2, q2s, q2s).wait_send()
    whole(s3.at[:, pl.ds(0, outer - 1)], q3s, q3s).wait_send()


def on_device(
    sp_size, tp_size, query, forget_logits, written_values, output_gate_logits, forget_floor_gap,
    extra_log_decay, head_norm_gain, output_weight, residual, mixer_norm_gain, mixer_up_weight,
    mixer_down_weight,
):
    rows, depth = residual.shape
    length, local_width = query.shape
    heads = local_width // HEAD_K
    depth_part, cols = mixer_up_weight.shape
    down_rows = mixer_down_weight.shape[0]
    inner, hi = sp_size // OUTER, tp_size // LO
    width = cols // OUTER
    up_pieces = max(1, min(2, depth_part // 128))
    down_pieces = max(1, min(2, down_rows // 64))
    steps = len(doubling(sp_size))
    f32, b16 = jnp.float32, jnp.bfloat16
    dma = pltpu.SemaphoreType.DMA
    vm = pltpu.VMEM
    O, F, C, half = OUTER, pieces_of(rows), halves_of(rows), depth // 2
    lrows = 8 * ((heads + 7) // 8)
    return pl.pallas_call(
        functools.partial(layer_kernel, sp_size, tp_size, up_pieces, down_pieces),
        out_shape=jax.ShapeDtypeStruct((rows, depth), b16),
        in_specs=[pl.BlockSpec(memory_space=pltpu.HBM)] * 12,
        out_specs=pl.BlockSpec(memory_space=pltpu.VMEM),
        scratch_shapes=[
            vm((length, local_width), b16), vm((length, local_width), b16),
            vm((length, local_width), b16), vm((length, local_width), b16),
            vm((length, local_width), f32),
            vm((1, local_width), f32), vm((1, HEAD_V), f32), vm((1, depth), f32),
            vm((rows, depth), b16),
            vm((length, local_width), f32), vm((length, local_width), f32),
            vm((length, local_width), f32), vm((length, local_width), b16),
            vm((heads, HEAD_V, HEAD_K), f32), vm((lrows, HEAD_K), f32),
            vm((heads, HEAD_V, HEAD_K), f32), vm((lrows, HEAD_K), f32),
            vm((steps, heads, HEAD_V, HEAD_K), b16), vm((steps, lrows, HEAD_K), f32),
            vm((steps, heads, HEAD_V, HEAD_K), b16), vm((steps, lrows, HEAD_K), f32),
            vm((tp_size, rows, local_width), b16), vm((LO, hi, rows, local_width), b16),
            vm((LO, local_width, depth), b16),
            vm((sp_size, depth_part, width), b16),
            vm((inner, down_rows, depth), b16),
            vm((hi, rows, depth), b16), vm((hi, rows, depth), b16),
            vm((rows, depth), f32),
            vm((O, tp_size, rows, depth), b16),
            vm((O, tp_size * rows, width), b16),
            vm((tp_size, rows, half), f32),
            vm((2 * O, hi, rows, half), f32),
            vm((2 * O, hi, rows, half), b16), vm((2 * O, hi, rows, half), b16),
            vm((2 * O, hi - 1, rows, half), b16), vm((2 * O, hi - 1, rows, half), b16),
            vm((2 * O, rows, half), f32),
            vm((2, O, rows, half), b16), vm((2, O + 1, rows, half), b16),
            dma((12,)),
            dma((steps,)), dma((steps,)), dma((steps,)), dma((steps,)),
            dma, dma, dma, dma,
            dma, dma((hi - 1, F)),
            dma, dma((O, up_pieces)),
            dma, dma, dma, dma((2,)),
            dma((O, 2)), dma((O, F)),
            dma, dma((O, hi - 1, F)),
            dma, dma((O,)),
            dma, dma((2 * O,)), dma, dma((2 * O, hi - 1, C)),
            dma, dma((2, O + 1, C)),
        ],
        compiler_params=pltpu.CompilerParams(
            collective_id=0, has_side_effects=True, vmem_limit_bytes=60 * 1024 * 1024
        ),
    )(
        query, forget_logits, written_values, output_gate_logits, forget_floor_gap.reshape(1, -1),
        extra_log_decay, head_norm_gain.reshape(1, -1), output_weight, residual,
        mixer_norm_gain.reshape(1, -1), mixer_up_weight, mixer_down_weight,
    )


def solution(mesh):
    return jax.shard_map(
        functools.partial(on_device, mesh.shape["sp"], mesh.shape["tp"]),
        mesh=mesh,
        in_specs=(
            P("sp", "tp"),
            P("sp", "tp"),
            P("sp", "tp"),
            P("sp", "tp"),
            P("tp"),
            P("sp", "tp"),
            P(),
            P("tp", None),
            P(("sp", "tp"), None),
            P(),
            P("sp", "tp"),
            P(("tp", "sp"), None),
        ),
        out_specs=P(("sp", "tp"), None),
        check_vma=False,
    )
```
